32 devices in a mesh: sp: 8 (over z, y), tp: 4 (over x, core).
Axes of the slice: x: 2, y: 2, z: 4, core: 2. Of those that a mesh axis runs over, the one named last changes fastest.
Arguments:
- tokens: bfloat16 [1024, 1024], P('sp', 'tp'), may hold values from -6 to 6
- norm_gain: float32 [1024], replicated, may hold values from 0.1 to 1.9
- attn_query: bfloat16 [1024, 512], P('sp', 'tp'), may hold values from -0.1875 to 0.1875
- attn_key: bfloat16 [1024, 256], P('sp', 'tp'), may hold values from -0.1875 to 0.1875
- attn_value: bfloat16 [1024, 256], P('sp', 'tp'), may hold values from -0.1875 to 0.1875
- sink_logit: float32 [8], P('tp'), may hold values from 2 to 7
- delta_query: bfloat16 [1024, 512], P('sp', 'tp'), may hold values from -0.1875 to 0.1875
- delta_key: bfloat16 [1024, 512], P('sp', 'tp'), may hold values from -0.1875 to 0.1875
- delta_value: bfloat16 [1024, 512], P('sp', 'tp'), may hold values from -0.1875 to 0.1875
- delta_gate: bfloat16 [1024, 512], P('sp', 'tp'), may hold values from -0.1875 to 0.1875
- beta_weight: bfloat16 [1024, 8, 2], P('sp', 'tp'), may hold values from -0.1875 to 0.1875
- decay_weight: bfloat16 [1024, 8, 2], P('sp', 'tp'), may hold values from -0.1875 to 0.1875
- beta_shift: float32 [2, 8], P(None, 'tp'), may hold values from -5 to -2
- decay_log: float32 [2, 8], P(None, 'tp'), may hold values from -2.5 to 1
- out_gain: float32 [64], replicated, may hold values from 0.1 to 1.9
- attn_out: bfloat16 [512, 1024], P('tp', 'sp'), may hold values from -1.5 to 1.5
- delta_out: bfloat16 [512, 1024], P('tp', 'sp'), may hold values from -0.25 to 0.25
Outputs:
- mixed: bfloat16 [1024, 1024], P(('sp', 'tp'))
The draws below stay inside these ranges and needn't reach their ends.
All inputs are finite; a program needn't handle non-finite values.
Results may differ from the reference program's by a relative error of at most 0.0045.
Values may be sent and summed in bfloat16 or wider, within the bound.
A program may use at most 64 MiB of HBM per device.

```python
import jax
import jax.numpy as jnp
from jax import lax

D = 1024
HEAD_DIM = 64
HEADS = 8
KV_HEADS = 4
DELTA_HEADS = 8
WINDOW = 64
TOK_DEV = 128
TOKENS = 1024
N_SP = 8


def shard_levels(stream_key, dims, split, low, largest):
    level, own = 1.0, jax.random.fold_in(stream_key, 6)
    for position, blocks in split:
        steps = jnp.exp(jax.random.uniform(jax.random.fold_in(own, position), (blocks,), jnp.float32, low / len(split), largest / len(split)))
        level = level * jnp.repeat(steps, dims[position] // blocks).reshape([-1 if axis == position else 1 for axis in range(len(dims))])
    return level


def noise(key, dims, scale, bound, shards=(), kind=jnp.bfloat16):
    entries = scale * jax.random.normal(key, dims, jnp.float32)
    if shards:
        entries = entries * shard_levels(key, dims, shards, -0.22, 0.18)
    return jnp.clip(entries, -bound, bound).astype(kind)


def setup_inputs(seed: int = 0) -> dict:
    key_of = jax.random.split(jax.random.key(seed), 18)
    tokens = noise(key_of[0], (TOKENS, D), 1.0, 6.0, ((0, 8), (1, 4)))
    norm_gain = jnp.clip(1.0 + 0.18 * jax.random.normal(key_of[1], (D,), jnp.float32), 0.1, 1.9)
    attn_query = noise(key_of[2], (D, HEADS * HEAD_DIM), D ** -0.5, 0.1875, ((0, 8), (1, 4)))
    attn_key = noise(key_of[3], (D, KV_HEADS * HEAD_DIM), D ** -0.5, 0.1875, ((0, 8), (1, 4)))
    attn_value = noise(key_of[4], (D, KV_HEADS * HEAD_DIM), D ** -0.5, 0.1875, ((0, 8), (1, 4)))
    sink_logit = jnp.clip(2.0 + 5.0 * jax.random.uniform(key_of[5], (HEADS,), jnp.float32) ** shard_levels(key_of[5], (HEADS,), ((0, 4),), -0.2, 0.2), 2.0, 7.0)
    delta_query = noise(key_of[6], (D, DELTA_HEADS * HEAD_DIM), D ** -0.5, 0.1875, ((0, 8), (1, 4)))
    delta_key = noise(key_of[7], (D, DELTA_HEADS * HEAD_DIM), D ** -0.5, 0.1875, ((0, 8), (1, 4)))
    delta_value = noise(key_of[8], (D, DELTA_HEADS * HEAD_DIM), D ** -0.5, 0.1875, ((0, 8), (1, 4)))
    delta_gate = noise(key_of[9], (D, DELTA_HEADS * HEAD_DIM), D ** -0.5, 0.1875, ((0, 8), (1, 4)))
    beta_weight = noise(key_of[10], (D, DELTA_HEADS, 2), D ** -0.5, 0.1875, ((0, 8), (1, 4)))
    decay_weight = noise(key_of[11], (D, DELTA_HEADS, 2), D ** -0.5, 0.1875, ((0, 8), (1, 4)))
    beta_shift = jnp.clip(-5.0 + 3.0 * jax.random.uniform(key_of[12], (2, DELTA_HEADS), jnp.float32) ** shard_levels(key_of[12], (2, DELTA_HEADS), ((1, 4),), -0.2, 0.2), -5.0, -2.0)
    decay_log = jnp.clip(-2.5 + 3.5 * jax.random.uniform(key_of[13], (2, DELTA_HEADS), jnp.float32) ** shard_levels(key_of[13], (2, DELTA_HEADS), ((1, 4),), -0.2, 0.2), -2.5, 1.0)
    out_gain = jnp.clip(1.0 + 0.18 * jax.random.normal(key_of[14], (HEAD_DIM,), jnp.float32), 0.1, 1.9)
    attn_out = noise(key_of[15], (HEADS * HEAD_DIM, D), 16 ** -0.5, 1.5, ((0, 4), (1, 8)))
    delta_out = noise(key_of[16], (DELTA_HEADS * HEAD_DIM, D), (DELTA_HEADS * HEAD_DIM) ** -0.5, 0.25, ((0, 4), (1, 8)))
    return {"tokens": tokens, "norm_gain": norm_gain, "attn_query": attn_query, "attn_key": attn_key, "attn_value": attn_value, "sink_logit": sink_logit, "delta_query": delta_query, "delta_key": delta_key, "delta_value": delta_value, "delta_gate": delta_gate, "beta_weight": beta_weight, "decay_weight": decay_weight, "beta_shift": beta_shift, "decay_log": decay_log, "out_gain": out_gain, "attn_out": attn_out, "delta_out": delta_out}


norm_eps = 1e-06

def rounded(values):
    return lax.optimization_barrier(values.astype(jnp.bfloat16))

def unit_rows(values):
    return values * lax.rsqrt(lax.optimization_barrier(jnp.sum(values * values, axis=-1, keepdims=True)) + norm_eps)

def delta_recur(queries, key_rows, value_rows, log_decay, strength):

    def advance(carry_state, inputs):
        q_row, k_row, v_row, g_row, b_row = inputs
        recall = jnp.einsum('hd,hde->he', k_row, carry_state, precision=lax.Precision.HIGHEST)
        beta_col = b_row[:, None, None]
        carry_state = jnp.exp(g_row)[:, None, None] * (carry_state - beta_col * k_row[:, :, None] * recall[:, None, :]) + beta_col * k_row[:, :, None] * v_row[:, None, :]
        output = jnp.einsum('hd,hde->he', q_row, carry_state, precision=lax.Precision.HIGHEST)
        return (carry_state, output)
    start_state = jnp.zeros((queries.shape[1], queries.shape[2], value_rows.shape[2]), jnp.float32)
    _, outputs = lax.scan(advance, start_state, (queries, key_rows, value_rows, log_decay, strength))
    return outputs

def reference(tokens, norm_gain, attn_query, attn_key, attn_value, sink_logit, delta_query, delta_key, delta_value, delta_gate, beta_weight, decay_weight, beta_shift, decay_log, out_gain, attn_out, delta_out):
    total_rows = tokens.shape[0]
    wide_rows = tokens.astype(jnp.float32)
    inverse = lax.rsqrt(lax.optimization_barrier(jnp.mean(wide_rows * wide_rows, axis=-1, keepdims=True)) + norm_eps)
    normed = (wide_rows * inverse * norm_gain).astype(jnp.bfloat16)

    def project(weight):
        return jnp.dot(normed, weight.reshape(weight.shape[0], -1), preferred_element_type=jnp.float32)
    group_size = HEADS // KV_HEADS
    queries = rounded(project(attn_query)).reshape(total_rows, KV_HEADS, group_size, HEAD_DIM)
    key_rows = rounded(project(attn_key)).reshape(total_rows, KV_HEADS, HEAD_DIM)
    value_rows = rounded(project(attn_value)).reshape(total_rows, KV_HEADS, HEAD_DIM)
    key_pad = jnp.pad(key_rows, ((WINDOW, WINDOW), (0, 0), (0, 0)))
    value_pad = jnp.pad(value_rows, ((WINDOW, WINDOW), (0, 0), (0, 0)))
    sink_row = sink_logit.reshape(KV_HEADS, group_size, 1, 1)
    key_span = TOK_DEV + 2 * WINDOW

    def attend(block_index):
        first_row = block_index * TOK_DEV
        q_block = lax.dynamic_slice_in_dim(queries, first_row, TOK_DEV, 0).astype(jnp.float32)
        k_block = lax.dynamic_slice_in_dim(key_pad, first_row, key_span, 0).astype(jnp.float32)
        v_block = lax.dynamic_slice_in_dim(value_pad, first_row, key_span, 0).astype(jnp.float32)
        scores = jnp.einsum('tkgd,jkd->kgtj', q_block, k_block) * HEAD_DIM ** (-0.5)
        q_pos = first_row + jnp.arange(TOK_DEV, dtype=jnp.int32)
        k_pos = first_row - WINDOW + jnp.arange(key_span, dtype=jnp.int32)
        allowed = (jnp.abs(q_pos[:, None] - k_pos[None, :]) <= WINDOW) & (k_pos[None, :] >= 0) & (k_pos[None, :] < total_rows)
        scores = jnp.where(allowed, scores, -jnp.inf)
        row_max = jnp.maximum(lax.optimization_barrier(jnp.max(scores, axis=-1, keepdims=True)), sink_row)
        weights = jnp.exp(scores - row_max)
        weights = weights / (lax.optimization_barrier(jnp.sum(weights, axis=-1, keepdims=True)) + jnp.exp(sink_row - row_max))
        heads_out = jnp.einsum('kgtj,jkd->tkgd', rounded(weights).astype(jnp.float32), v_block)
        return heads_out.reshape(TOK_DEV, HEADS * HEAD_DIM).astype(jnp.bfloat16)
    y_attn = lax.map(attend, jnp.arange(N_SP, dtype=jnp.int32)).reshape(total_rows, HEADS * HEAD_DIM)

    def activate(weight):
        return jax.nn.silu(rounded(project(weight)).astype(jnp.float32)).reshape(total_rows, DELTA_HEADS, HEAD_DIM)
    d_query = unit_rows(activate(delta_query)) * HEAD_DIM ** (-0.5)
    d_key = unit_rows(activate(delta_key))
    d_value = activate(delta_value)
    gate_rows = rounded(project(delta_gate)).astype(jnp.float32).reshape(total_rows, DELTA_HEADS, HEAD_DIM)
    strength = jax.nn.sigmoid(project(beta_weight).reshape(total_rows, DELTA_HEADS, 2) + beta_shift.T)
    log_decay = -jnp.exp(decay_log.T) * jax.nn.softplus(project(decay_weight).reshape(total_rows, DELTA_HEADS, 2)) / total_rows
    forward = delta_recur(d_query, d_key, d_value, log_decay[:, :, 0], strength[:, :, 0])
    backward = jnp.flip(delta_recur(jnp.flip(d_query, 0), jnp.flip(d_key, 0), jnp.flip(d_value, 0), jnp.flip(log_decay[:, :, 1], 0), jnp.flip(strength[:, :, 1], 0)), 0)
    both_ways = forward + backward
    normed_out = both_ways * lax.rsqrt(lax.optimization_barrier(jnp.mean(both_ways * both_ways, axis=-1, keepdims=True)) + norm_eps) * out_gain
    y_delta = (normed_out * jax.nn.silu(gate_rows)).astype(jnp.bfloat16).reshape(total_rows, DELTA_HEADS * HEAD_DIM)
    summed = jnp.dot(y_attn, attn_out, preferred_element_type=jnp.float32) + jnp.dot(y_delta, delta_out, preferred_element_type=jnp.float32)
    return summed.astype(jnp.bfloat16)
```

```python
import functools

import jax
import jax.numpy as jnp
from jax import lax
from jax.experimental import pallas as pl
from jax.experimental.pallas import tpu as pltpu
from jax.sharding import PartitionSpec as P

HEAD_DIM = 64
WINDOW = 64
norm_eps = 1e-06
MESH = pl.DeviceIdType.MESH
F32 = jnp.float32
BF16 = jnp.bfloat16
SUM_DTYPE = jnp.float32


def exact(a, b, dims=((1,), (0,))):
    return lax.dot_general(
        a, b, (dims, ((), ())), precision=lax.Precision.HIGHEST, preferred_element_type=F32
    )


def plain(a, b, dims=((1,), (0,))):
    return lax.dot_general(a, b, (dims, ((), ())), preferred_element_type=F32)


def silu(x):
    return x * jax.nn.sigmoid(x)


def unit_rows(x):
    return x * lax.rsqrt(jnp.sum(x * x, axis=-1, keepdims=True) + norm_eps)


def copy_to(src, dst, send, recv, device):
    return pltpu.make_async_remote_copy(
        src_ref=src,
        dst_ref=dst,
        send_sem=send,
        recv_sem=recv,
        device_id=device,
        device_id_type=MESH,
    )


class Gather:
    def __init__(self, n, me, tp, own, buf, send, recv):
        self.nh = n // 2
        self.me, self.tp = me, tp
        self.lo, self.hi = lax.rem(me, 2), lax.div(me, 2)
        self.own, self.buf, self.send, self.recv = own, buf, send, recv

    def copy(self, b, route, own=False):
        target = (self.me + 2, self.me - 2, self.hi * 2 + 1 - self.lo)[route]
        return copy_to(
            self.own if own else self.buf.at[b],
            self.buf.at[b],
            self.send.at[route, b],
            self.recv.at[b],
            (target, self.tp),
        )

    def can(self, route):
        return self.hi < self.nh - 1 if route == 0 else self.hi > 0

    def begin(self):
        self.copy(self.me, 2, True).start()
        for route in (0, 1):

            @pl.when(self.can(route))
            def _(route=route):
                self.copy(self.me, route, True).start()

    def take(self, b, use):
        self.copy(b, 2).wait_recv()
        if use is not None:
            use(b)

    def step(self, d, use=None):
        if d < self.nh:
            for route, there, ok in (
                (0, self.hi - d, self.hi - d >= 0),
                (1, self.hi + d, self.hi + d < self.nh),
            ):

                @pl.when(ok)
                def _(route=route, there=there):
                    b = there * 2 + self.lo
                    self.copy(b, 2).wait_recv()

                    @pl.when(self.can(route))
                    def _():
                        self.copy(b, route).start()

                    self.copy(b, 2).start()
                    if use is not None:
                        use(b)

        e = d - 1
        if e == 0:
            self.take(self.hi * 2 + 1 - self.lo, use)
        else:
            for there, ok in (
                (self.hi - e, self.hi - e >= 0),
                (self.hi + e, self.hi + e < self.nh),
            ):

                @pl.when(ok)
                def _(there=there):
                    self.take(there * 2 + 1 - self.lo, use)

    def drain(self):
        self.copy(self.me, 2, True).wait_send()
        for route in (0, 1):

            @pl.when(self.can(route))
            def _(route=route):
                self.copy(self.me, route, True).wait_send()

        for d in range(1, self.nh):
            for route, there, ok in (
                (0, self.hi - d, self.hi - d >= 0),
                (1, self.hi + d, self.hi + d < self.nh),
            ):

                @pl.when(ok)
                def _(route=route, there=there):
                    b = there * 2 + self.lo

                    @pl.when(self.can(route))
                    def _():
                        self.copy(b, route).wait_send()

                    self.copy(b, 2).wait_send()


def layer_kernel(
    n, nt, heads, kvs, dheads,
    tok, gain, wp, wo, par, og, out,
    tokbuf, normed, wbuf, obuf, acc, kvbuf, st, stbuf, o_loc, r_mat, joined, part, rsbuf,
    tok_s, tok_r, w_s, w_r, o_s, o_r, kv_s, kv_r, st_s, st_r, rs_s, rs_r,
):
    me, t = lax.axis_index("sp"), lax.axis_index("tp")
    rows, width = tok.shape
    kb = wp.shape[0]
    hd = HEAD_DIM
    bar = pltpu.get_barrier_semaphore()
    for d in range(1, n):
        pl.semaphore_signal(bar, inc=1, device_id=(lax.rem(me + d, n), t), device_id_type=MESH)
    for d in range(1, nt):
        pl.semaphore_signal(bar, inc=1, device_id=(me, lax.rem(t + d, nt)), device_id_type=MESH)
    pl.semaphore_wait(bar, n - 1 + nt - 1)

    tok_copies = [
        copy_to(tok, tokbuf.at[t], tok_s.at[d - 1], tok_r.at[t], (me, lax.rem(t + d, nt)))
        for d in range(1, nt)
    ]
    for c in tok_copies:
        c.start()
    wg = Gather(n, me, t, wp, wbuf, w_s, w_r)
    ogather = Gather(n, me, t, wo, obuf, o_s, o_r)
    wg.begin()
    tokbuf[t] = tok[...]
    obuf[me] = wo[...]
    for d in range(1, nt):
        j = lax.rem(t + d, nt)
        copy_to(tok, tokbuf.at[j], tok_s.at[d - 1], tok_r.at[j], (me, j)).wait_recv()
    total = jnp.zeros((rows, 1), F32)
    for j in range(nt):
        x = tokbuf[j].astype(F32)
        total += jnp.sum(x * x, axis=-1, keepdims=True)
    inverse = lax.rsqrt(total / (nt * width) + norm_eps)
    per = width // kb
    for j in range(nt):
        x = (tokbuf[j].astype(F32) * inverse * gain[j : j + 1, :]).astype(BF16)
        for i in range(per):
            normed[j * per + i] = x[:, i * kb : (i + 1) * kb]
    acc[...] = plain(normed[me], wp[...])

    def use(b):
        acc[...] += plain(normed[b], wbuf[b])

    for d in range(1, n // 2 + 1):
        wg.step(d, use)
    ogather.begin()

    aw, kw, dw = heads * hd, kvs * hd, dheads * hd
    kvbuf[WINDOW : WINDOW + rows] = acc[:, aw : aw + 2 * kw].astype(BF16)

    @pl.when(me == 0)
    def _():
        kvbuf[:WINDOW] = jnp.zeros((WINDOW, 2 * kw), BF16)

    @pl.when(me == n - 1)
    def _():
        kvbuf[WINDOW + rows :] = jnp.zeros((WINDOW, 2 * kw), BF16)

    base = aw + 2 * kw
    tail = acc[:, base + 4 * dw :]
    beta_all = jax.nn.sigmoid(tail + par[0:1, :])
    soft = jnp.maximum(tail, 0.0) + jnp.log1p(jnp.exp(-jnp.abs(tail)))
    g_all = par[1:2, :] * soft
    ri = lax.broadcasted_iota(jnp.int32, (rows, rows), 0)
    ci = lax.broadcasted_iota(jnp.int32, (rows, rows), 1)
    incl = (ri >= ci, ri <= ci)
    strict = (ri > ci, ri < ci)
    cum = [exact(jnp.where(m, 1.0, 0.0).astype(F32), g_all) for m in incl]
    cum_t = [c.T for c in cum]

    def head_to(p):
        up = copy_to(
            kvbuf.at[pl.ds(rows, WINDOW)], kvbuf.at[pl.ds(0, WINDOW)],
            kv_s.at[0], kv_r.at[0], (me + 1, t),
        )
        down = copy_to(
            kvbuf.at[pl.ds(WINDOW, WINDOW)], kvbuf.at[pl.ds(WINDOW + rows, WINDOW)],
            kv_s.at[1], kv_r.at[1], (me - 1, t),
        )
        return (up, down)[p]

    pl.when(me < n - 1)(lambda: head_to(0).start())
    pl.when(me > 0)(lambda: head_to(1).start())

    chains = []
    qs = []
    for h in range(dheads):
        def cols(i):
            lo_c = base + i * dw + h * hd
            return acc[:, lo_c : lo_c + hd].astype(BF16).astype(F32)

        q = unit_rows(silu(cols(0))) * hd ** (-0.5)
        k = unit_rows(silu(cols(1)))
        v = silu(cols(2))
        kk = exact(k, k, ((1,), (1,)))
        qk = exact(q, k, ((1,), (1,)))
        for r in range(2):
            c = h * 2 + r
            lane = 2 * dheads + c
            gcol = cum[r][:, lane : lane + 1]
            grow = cum_t[r][lane : lane + 1, :]
            beta = beta_all[:, c : c + 1]
            decay = jnp.where(incl[r], jnp.exp(jnp.minimum(gcol - grow, 0.0)), 0.0)
            a = jnp.where(strict[r], beta * kk * decay, 0.0)
            eg = jnp.exp(gcol)
            last = gcol[rows - 1 : rows, :] if r == 0 else gcol[0:1, :]
            chains.append(
                dict(
                    r=r, h=h, a=a, rhs=jnp.concatenate([beta * v, beta * k * eg], axis=1),
                    pm=qk * decay, qe=q * eg, kd=(k * jnp.exp(last - gcol)).T, last=last,
                )
            )
    size = 1
    while (1 << size) <= rows:
        size += 1
    levels = size - 1
    eye = jnp.where(ri == ci, 1.0, 0.0).astype(F32)
    xor = ri ^ ci
    inv = [eye - jnp.where(xor == 1, ch["a"], 0.0) for ch in chains]
    for lv in range(1, levels):
        m = (xor >> lv) == 1
        left = [exact(x, jnp.where(m, ch["a"], 0.0)) for x, ch in zip(inv, chains)]
        inv = [x - exact(y, x) for x, y in zip(inv, left)]
    sols = [exact(x, ch["rhs"]) for x, ch in zip(inv, chains)]
    outs = [exact(ch["kd"], s) for ch, s in zip(chains, sols)]
    e64 = jnp.where(
        lax.broadcasted_iota(jnp.int32, (hd, hd), 0)
        == lax.broadcasted_iota(jnp.int32, (hd, hd), 1), 1.0, 0.0,
    ).astype(F32)
    for ch, s in zip(chains, outs):
        st[ch["r"], ch["h"], :, :hd] = s[:, :hd]
        st[ch["r"], ch["h"], :, hd:] = jnp.exp(ch["last"]) * e64 - s[:, hd:]
    inner = [exact(ch["pm"], s) for ch, s in zip(chains, sols)]
    for ch, s in zip(chains, inner):
        o_loc[ch["r"], ch["h"]] = s[:, :hd]
        r_mat[ch["r"], ch["h"]] = ch["qe"] - s[:, hd:]

    def state_copy(r, p):
        return copy_to(st.at[r], stbuf.at[me], st_s.at[p], st_r.at[me], (p, t))

    def state_all(act):
        for d in range(n - 1, 0, -1):
            pl.when(me + d < n)(lambda d=d: act(state_copy(0, me + d)))
            pl.when(me - d >= 0)(lambda d=d: act(state_copy(1, me - d)))

    state_all(lambda c: c.start())
    ogather.step(1)

    pl.when(me > 0)(lambda: head_to(0).wait_recv())
    pl.when(me < n - 1)(lambda: head_to(1).wait_recv())
    span = rows + 2 * WINDOW
    qi = lax.broadcasted_iota(jnp.int32, (rows, span), 0)
    kj = lax.broadcasted_iota(jnp.int32, (rows, span), 1) - WINDOW
    pos = kj + me * rows
    allowed = (jnp.abs(qi - kj) <= WINDOW) & (pos >= 0) & (pos < n * rows)
    for h in range(heads):
        g = h // (heads // kvs)
        q = acc[:, h * hd : (h + 1) * hd].astype(BF16)
        s = plain(q, kvbuf[:, g * hd : (g + 1) * hd], ((1,), (1,))) * hd ** (-0.5)
        s = jnp.where(allowed, s, -jnp.inf)
        sink = par[2:3, h : h + 1]
        m = jnp.maximum(jnp.max(s, axis=-1, keepdims=True), sink)
        e = jnp.exp(s - m)
        p = e / (jnp.sum(e, axis=-1, keepdims=True) + jnp.exp(sink - m))
        o = plain(p.astype(BF16), kvbuf[:, kw + g * hd : kw + (g + 1) * hd])
        joined[:, h * hd : (h + 1) * hd] = o.astype(BF16)
    for d in range(2, n // 2 + 1):
        ogather.step(d)

    for i in range(n):

        @pl.when(me != i)
        def _(i=i):
            copy_to(st.at[0], stbuf.at[i], st_s.at[i], st_r.at[i], (me, t)).wait_recv()

    fore = [jnp.zeros((hd, hd), F32)] * dheads
    back = [jnp.zeros((hd, hd), F32)] * dheads

    def enter(i, state, h, ok):
        both = jnp.where(ok, stbuf[i, h], ident)
        return exact(both[:, hd:], state) + both[:, :hd]

    ident = jnp.concatenate([jnp.zeros((hd, hd), F32), e64], axis=1)
    for i in range(n - 1):
        fore = [enter(i, x, h, i < me) for h, x in enumerate(fore)]
        back = [enter(n - 1 - i, x, h, n - 1 - i > me) for h, x in enumerate(back)]
    for h in range(dheads):
        o = o_loc[0, h] + o_loc[1, h] + exact(r_mat[0, h], fore[h]) + exact(r_mat[1, h], back[h])
        o = o * lax.rsqrt(jnp.mean(o * o, axis=-1, keepdims=True) + norm_eps) * og[...]
        lo_c = base + 3 * dw + h * hd
        gate = acc[:, lo_c : lo_c + hd].astype(BF16).astype(F32)
        joined[:, aw + h * hd : aw + (h + 1) * hd] = (o * silu(gate)).astype(BF16)

    cw = wo.shape[1]
    tr = rows // nt
    lhs = joined[...]
    for b in range(n):
        y = plain(lhs, obuf[b])
        for j in range(nt):
            part[j, :, b * cw : (b + 1) * cw] = y[j * tr : (j + 1) * tr].astype(SUM_DTYPE)
    rs_copies = [
        copy_to(
            part.at[lax.rem(t + d, nt)], rsbuf.at[d - 1], rs_s.at[d - 1], rs_r.at[d - 1],
            (me, lax.rem(t + d, nt)),
        )
        for d in range(1, nt)
    ]
    for c in rs_copies:
        c.start()
    for c in tok_copies:
        c.wait_send()
    wg.drain()
    ogather.drain()
    pl.when(me < n - 1)(lambda: head_to(0).wait_send())
    pl.when(me > 0)(lambda: head_to(1).wait_send())
    state_all(lambda c: c.wait_send())
    total = part[t].astype(F32)
    for d in range(1, nt):
        rs_copies[d - 1].wait_recv()
        total += rsbuf[d - 1].astype(F32)
    out[...] = total.astype(BF16)
    for c in rs_copies:
        c.wait_send()


def per_device(
    tokens, norm_gain, attn_query, attn_key, attn_value, sink_logit, delta_query, delta_key,
    delta_value, delta_gate, beta_weight, decay_weight, beta_shift, decay_log, out_gain,
    attn_out, delta_out,
):
    n, nt = lax.axis_size("sp"), lax.axis_size("tp")
    rows, width = tokens.shape
    kb = attn_query.shape[0]
    heads, kvs = attn_query.shape[1] // HEAD_DIM, attn_key.shape[1] // HEAD_DIM
    dheads = delta_query.shape[1] // HEAD_DIM
    ab = 2 * dheads
    wp = jnp.concatenate(
        [
            attn_query, attn_key, attn_value, delta_query, delta_key, delta_value, delta_gate,
            beta_weight.reshape(kb, ab), decay_weight.reshape(kb, ab),
            jnp.zeros((kb, 128 - 2 * ab), BF16),
        ],
        axis=1,
    )
    wo = jnp.concatenate([attn_out, delta_out], axis=0)
    flat = lambda a: a.T.reshape(1, ab)
    par = jnp.concatenate(
        [
            jnp.pad(flat(beta_shift), ((0, 0), (0, 128 - ab))),
            jnp.pad(-jnp.exp(flat(decay_log)) / (rows * n), ((0, 0), (ab, 128 - 2 * ab))),
            jnp.pad(sink_logit.reshape(1, heads), ((0, 0), (0, 128 - heads))),
            jnp.zeros((5, 128), F32),
        ],
        axis=0,
    )
    cw = wo.shape[1]
    tr = rows // nt
    hd = HEAD_DIM
    kw = kvs * hd
    dma = pltpu.SemaphoreType.DMA
    vm = pl.BlockSpec(memory_space=pltpu.VMEM)
    return pl.pallas_call(
        functools.partial(layer_kernel, n, nt, heads, kvs, dheads),
        out_shape=jax.ShapeDtypeStruct((tr, n * cw), BF16),
        in_specs=[vm] * 6,
        out_specs=vm,
        scratch_shapes=[
            pltpu.VMEM((nt, rows, width), BF16),
            pltpu.VMEM((n, rows, kb), BF16),
            pltpu.VMEM((n,) + wp.shape, BF16),
            pltpu.VMEM((n,) + wo.shape, BF16),
            pltpu.VMEM((rows, wp.shape[1]), F32),
            pltpu.VMEM((rows + 2 * WINDOW, 2 * kw), BF16),
            pltpu.VMEM((2, dheads, hd, 2 * hd), F32),
            pltpu.VMEM((n, dheads, hd, 2 * hd), F32),
            pltpu.VMEM((2, dheads, rows, hd), F32),
            pltpu.VMEM((2, dheads, rows, hd), F32),
            pltpu.VMEM((rows, (heads + dheads) * hd), BF16),
            pltpu.VMEM((nt, tr, n * cw), SUM_DTYPE),
            pltpu.VMEM((nt - 1, tr, n * cw), SUM_DTYPE),
            dma((nt - 1,)), dma((nt,)),
            dma((3, n)), dma((n,)),
            dma((3, n)), dma((n,)),
            dma((2,)), dma((2,)),
            dma((n,)), dma((n,)),
            dma((nt - 1,)), dma((nt - 1,)),
        ],
        compiler_params=pltpu.CompilerParams(
            collective_id=0, has_side_effects=True, vmem_limit_bytes=48 * 1024 * 1024
        ),
    )(tokens, norm_gain.reshape(nt, width), wp, wo, par, out_gain.reshape(1, hd))


def solution(mesh):
    return jax.shard_map(
        per_device,
        mesh=mesh,
        in_specs=(
            P("sp", "tp"), P(), P("sp", "tp"), P("sp", "tp"), P("sp", "tp"), P("tp"),
            P("sp", "tp"), P("sp", "tp"), P("sp", "tp"), P("sp", "tp"),
            P("sp", "tp", None), P("sp", "tp", None), P(None, "tp"), P(None, "tp"), P(),
            P("tp", "sp"), P("tp", "sp"),
        ),
        out_specs=P(("sp", "tp"), None),
        check_vma=False,
    )
```

```python
import functools

import jax
import jax.numpy as jnp
from jax import lax
from jax.experimental import pallas as pl
from jax.experimental.pallas import tpu as pltpu
from jax.sharding import PartitionSpec as P

HEAD_DIM = 64
WINDOW = 64
norm_eps = 1e-06
MESH = pl.DeviceIdType.MESH
F32 = jnp.float32
BF16 = jnp.bfloat16
SUM_DTYPE = jnp.bfloat16
PARTS = 2


def exact(a, b, dims=((1,), (0,))):
    return lax.dot_general(
        a, b, (dims, ((), ())), precision=lax.Precision.HIGHEST, preferred_element_type=F32
    )


def plain(a, b, dims=((1,), (0,))):
    return lax.dot_general(a, b, (dims, ((), ())), preferred_element_type=F32)


def split(x):
    high = x.astype(BF16)
    return high, (x - high.astype(F32)).astype(BF16)


def close(a, b, dims=((1,), (0,))):
    (ca,), (cb,) = dims
    left = jnp.concatenate([a[0], a[1], a[0]], axis=ca)
    right = jnp.concatenate([b[0], b[0], b[1]], axis=cb)
    return plain(left, right, dims)


def near(a, b, dims=((1,), (0,))):
    a, b = split(a), split(b)
    return plain(a[0], b[0], dims) + (plain(a[1], b[0], dims) + plain(a[0], b[1], dims))


def silu(x):
    return x * jax.nn.sigmoid(x)


def unit_rows(x):
    return x * lax.rsqrt(jnp.sum(x * x, axis=-1, keepdims=True) + norm_eps)


def copy_to(src, dst, send, recv, device):
    return pltpu.make_async_remote_copy(
        src_ref=src,
        dst_ref=dst,
        send_sem=send,
        recv_sem=recv,
        device_id=device,
        device_id_type=MESH,
    )


class Gather:
    def __init__(self, n, me, tp, own, buf, send, recv, parts):
        self.nh = n // 2
        self.me, self.tp = me, tp
        self.lo, self.hi = lax.rem(me, 2), lax.div(me, 2)
        self.own, self.buf, self.send, self.recv = own, buf, send, recv
        self.parts = parts
        self.size = own.shape[1] // parts

    def copy(self, b, route, p, own=False):
        target = (self.me + 2, self.me - 2, self.hi * 2 + 1 - self.lo)[route]
        cols = pl.ds(p * self.size, self.size)
        here = self.own.at[:, cols] if own else self.buf.at[b, :, cols]
        return copy_to(
            here,
            self.buf.at[b, :, cols],
            self.send.at[route, b, p],
            self.recv.at[b, p],
            (target, self.tp),
        )

    def can(self, route):
        return self.hi < self.nh - 1 if route == 0 else self.hi > 0

    def first(self, act):
        for p in range(self.parts):
            for route in (0, 1):
                pl.when(self.can(route))(lambda p=p, route=route: act(self.copy(self.me, route, p, True)))
            act(self.copy(self.me, 2, p, True))

    def begin(self):
        self.first(lambda c: c.start())

    def sides(self, d):
        return ((0, self.hi - d, self.hi - d >= 0), (1, self.hi + d, self.hi + d < self.nh))

    def step(self, d, use=None):
        for p in range(self.parts):
            if d < self.nh:
                for route, there, ok in self.sides(d):

                    @pl.when(ok)
                    def _(route=route, there=there):
                        b = there * 2 + self.lo
                        self.copy(b, 2, p).wait_recv()
                        pl.when(self.can(route))(lambda: self.copy(b, route, p).start())
                        self.copy(b, 2, p).start()
                        if use is not None:
                            use(b, p)

            for i, (_, there, ok) in enumerate(self.sides(d - 1)):
                if d == 1 and i == 1:
                    continue

                @pl.when(ok)
                def _(there=there):
                    b = there * 2 + 1 - self.lo
                    self.copy(b, 2, p).wait_recv()
                    if use is not None:
                        use(b, p)

    def drain(self):
        self.first(lambda c: c.wait_send())
        for d in range(1, self.nh):
            for p in range(self.parts):
                for route, there, ok in self.sides(d):

                    @pl.when(ok)
                    def _(route=route, there=there):
                        b = there * 2 + self.lo
                        pl.when(self.can(route))(lambda: self.copy(b, route, p).wait_send())
                        self.copy(b, 2, p).wait_send()


def layer_kernel(
    n, nt, heads, kvs, dheads,
    tok, gain, wp, wo, ab, par, og, out,
    tokbuf, normed, wbuf, obuf, abbuf, acc, kvbuf, st, stbuf, o_loc, r_mat, joined, part, rsbuf,
    tok_s, tok_r, w_s, w_r, o_s, o_r, ab_s, ab_r, kv_s, kv_r, st_s, st_r, rs_s, rs_r,
):
    me, t = lax.axis_index("sp"), lax.axis_index("tp")
    rows, width = tok.shape
    kb = wp.shape[0]
    hd = HEAD_DIM
    bar = pltpu.get_barrier_semaphore()
    for d in range(1, n):
        pl.semaphore_signal(bar, inc=1, device_id=(lax.rem(me + d, n), t), device_id_type=MESH)
    for d in range(1, nt):
        pl.semaphore_signal(bar, inc=1, device_id=(me, lax.rem(t + d, nt)), device_id_type=MESH)
    pl.semaphore_wait(bar, n - 1 + nt - 1)

    tok_copies = [
        copy_to(tok, tokbuf.at[t], tok_s.at[d - 1], tok_r.at[t], (me, lax.rem(t + d, nt)))
        for d in range(1, nt)
    ]
    for c in tok_copies:
        c.start()
    wg = Gather(n, me, t, wp, wbuf, w_s, w_r, PARTS)
    ogather = Gather(n, me, t, wo, obuf, o_s, o_r, 1)
    wg.begin()

    def ab_copy(d):
        p = lax.rem(me + d, n)
        return copy_to(ab, abbuf.at[me], ab_s.at[d], ab_r.at[me], (p, t))

    for d in range(1, n):
        ab_copy(d).start()
    abbuf[me] = ab[...]
    tokbuf[t] = tok[...]
    obuf[me] = wo[...]
    for d in range(1, nt):
        j = lax.rem(t + d, nt)
        copy_to(tok, tokbuf.at[j], tok_s.at[d - 1], tok_r.at[j], (me, j)).wait_recv()
    total = jnp.zeros((rows, 1), F32)
    for j in range(nt):
        x = tokbuf[j].astype(F32)
        total += jnp.sum(x * x, axis=-1, keepdims=True)
    inverse = lax.rsqrt(total / (nt * width) + norm_eps)
    per = width // kb
    for j in range(nt):
        x = (tokbuf[j].astype(F32) * inverse * gain[j : j + 1, :]).astype(BF16)
        for i in range(per):
            normed[j * per + i] = x[:, i * kb : (i + 1) * kb]
    acc[...] = plain(normed[me], wp[...])

    half = wp.shape[1] // PARTS

    def use(b, p):
        cols = slice(p * half, (p + 1) * half)
        acc[:, cols] += plain(normed[b], wbuf[b, :, cols])

    for d in range(1, n // 2 + 1):
        wg.step(d, use)
    ogather.begin()

    aw, kw, dw = heads * hd, kvs * hd, dheads * hd
    kvbuf[WINDOW : WINDOW + rows] = acc[:, aw : aw + 2 * kw].astype(BF16)

    @pl.when(me == 0)
    def _():
        kvbuf[:WINDOW] = jnp.zeros((WINDOW, 2 * kw), BF16)

    @pl.when(me == n - 1)
    def _():
        kvbuf[WINDOW + rows :] = jnp.zeros((WINDOW, 2 * kw), BF16)

    base = aw + 2 * kw
    for d in range(1, n):
        p = lax.rem(me + d, n)
        copy_to(ab, abbuf.at[p], ab_s.at[d], ab_r.at[p], (p, t)).wait_recv()
    tail = plain(abbuf[0], normed[0], ((1,), (1,)))
    for b in range(1, n):
        tail += plain(abbuf[b], normed[b], ((1,), (1,)))
    beta_t = jax.nn.sigmoid(tail + par[:, 0:1])
    soft = jnp.maximum(tail, 0.0) + jnp.log1p(jnp.exp(-jnp.abs(tail)))
    g_t = par[:, 1:2] * soft
    ri = lax.broadcasted_iota(jnp.int32, (rows, rows), 0)
    ci = lax.broadcasted_iota(jnp.int32, (rows, rows), 1)
    incl = (ri >= ci, ri <= ci)
    strict = (ri > ci, ri < ci)
    na = ab.shape[0]
    cum_t = [exact(g_t, jnp.where(m, 1.0, 0.0).astype(F32)) for m in (incl[1], incl[0])]
    stack = [beta_t] + cum_t
    if 3 * na < 128:
        stack.append(jnp.zeros((128 - 3 * na, rows), F32))
    columns = jnp.concatenate(stack, axis=0).T

    def head_to(p):
        up = copy_to(
            kvbuf.at[pl.ds(rows, WINDOW)], kvbuf.at[pl.ds(0, WINDOW)],
            kv_s.at[0], kv_r.at[0], (me + 1, t),
        )
        down = copy_to(
            kvbuf.at[pl.ds(WINDOW, WINDOW)], kvbuf.at[pl.ds(WINDOW + rows, WINDOW)],
            kv_s.at[1], kv_r.at[1], (me - 1, t),
        )
        return (up, down)[p]

    pl.when(me < n - 1)(lambda: head_to(0).start())
    pl.when(me > 0)(lambda: head_to(1).start())

    chains = []
    qs = []
    for h in range(dheads):
        def cols(i):
            lo_c = base + i * dw + h * hd
            return acc[:, lo_c : lo_c + hd].astype(BF16).astype(F32)

        q = unit_rows(silu(cols(0))) * hd ** (-0.5)
        k = unit_rows(silu(cols(1)))
        v = silu(cols(2))
        kk = near(k, k, ((1,), (1,)))
        qk = near(q, k, ((1,), (1,)))
        for r in range(2):
            c = h * 2 + r
            lane = 2 * dheads + c
            at = (1 + r) * na + lane
            gcol = columns[:, at : at + 1]
            grow = cum_t[r][lane : lane + 1, :]
            beta = columns[:, c : c + 1]
            decay = jnp.where(incl[r], jnp.exp(jnp.minimum(gcol - grow, 0.0)), 0.0)
            a = jnp.where(strict[r], beta * kk * decay, 0.0)
            eg = jnp.exp(gcol)
            last = gcol[rows - 1 : rows, :] if r == 0 else gcol[0:1, :]
            chains.append(
                dict(
                    r=r, h=h, a=a, rhs=jnp.concatenate([beta * v, beta * k * eg], axis=1),
                    pm=qk * decay, qe=q * eg, kd=(k * jnp.exp(last - gcol)).T, last=last,
                )
            )
    size = 1
    while (1 << size) <= rows:
        size += 1
    levels = size - 1
    eye = jnp.where(ri == ci, 1.0, 0.0).astype(F32)
    xor = ri ^ ci
    inv = [eye - jnp.where(xor == 1, ch["a"], 0.0) for ch in chains]
    pairs = [split(ch["a"]) for ch in chains]
    waits = {levels // 3 + i: i + 1 for i in range(n // 2)}
    for lv in range(1, levels):
        m = jnp.where((xor >> lv) == 1, 1.0, 0.0).astype(BF16)
        xs = [split(x) for x in inv]
        left = [close(x, (m * a[0], m * a[1])) for x, a in zip(xs, pairs)]
        inv = [x - close(split(y), z) for x, y, z in zip(inv, left, xs)]
        if lv in waits:
            ogather.step(waits[lv])
    done = sum(lv in waits for lv in range(1, levels))
    sols = [split(close(split(x), split(ch["rhs"]))) for x, ch in zip(inv, chains)]
    outs = [close(split(ch["kd"]), s) for ch, s in zip(chains, sols)]
    e64 = jnp.where(
        lax.broadcasted_iota(jnp.int32, (hd, hd), 0)
        == lax.broadcasted_iota(jnp.int32, (hd, hd), 1), 1.0, 0.0,
    ).astype(F32)
    for ch, s in zip(chains, outs):
        full = jnp.concatenate([s[:, :hd], jnp.exp(ch["last"]) * e64 - s[:, hd:]], axis=1)
        st[ch["r"], ch["h"]] = full.astype(BF16)
    def state_copy(r, p):
        return copy_to(st.at[r], stbuf.at[me], st_s.at[p], st_r.at[me], (p, t))

    def state_all(act):
        for d in range(n - 1, 0, -1):
            pl.when(me + d < n)(lambda d=d: act(state_copy(0, me + d)))
            pl.when(me - d >= 0)(lambda d=d: act(state_copy(1, me - d)))

    state_all(lambda c: c.start())
    inner = [close(split(ch["pm"]), s) for ch, s in zip(chains, sols)]
    for ch, s in zip(chains, inner):
        o_loc[ch["r"], ch["h"]] = s[:, :hd]
        r_mat[ch["r"], ch["h"]] = ch["qe"] - s[:, hd:]


    pl.when(me > 0)(lambda: head_to(0).wait_recv())
    pl.when(me < n - 1)(lambda: head_to(1).wait_recv())
    span = rows + 2 * WINDOW
    qi = lax.broadcasted_iota(jnp.int32, (rows, span), 0)
    kj = lax.broadcasted_iota(jnp.int32, (rows, span), 1) - WINDOW
    pos = kj + me * rows
    allowed = (jnp.abs(qi - kj) <= WINDOW) & (pos >= 0) & (pos < n * rows)
    for h in range(heads):
        g = h // (heads // kvs)
        q = acc[:, h * hd : (h + 1) * hd].astype(BF16)
        s = plain(q, kvbuf[:, g * hd : (g + 1) * hd], ((1,), (1,))) * hd ** (-0.5)
        s = jnp.where(allowed, s, -jnp.inf)
        sink = par[h : h + 1, 2:3]
        m = jnp.maximum(jnp.max(s, axis=-1, keepdims=True), sink)
        e = jnp.exp(s - m)
        p = e / (jnp.sum(e, axis=-1, keepdims=True) + jnp.exp(sink - m))
        o = plain(p.astype(BF16), kvbuf[:, kw + g * hd : kw + (g + 1) * hd])
        joined[:, h * hd : (h + 1) * hd] = o.astype(BF16)
    for d in range(done + 1, n // 2 + 1):
        ogather.step(d)

    for i in range(n):

        @pl.when(me != i)
        def _(i=i):
            copy_to(st.at[0], stbuf.at[i], st_s.at[i], st_r.at[i], (me, t)).wait_recv()

    fore = [jnp.zeros((hd, hd), F32)] * dheads
    back = [jnp.zeros((hd, hd), F32)] * dheads

    def enter(i, state, h, ok):
        both = jnp.where(ok, stbuf[i, h].astype(F32), ident)
        move, (high, low) = both[:, hd:].astype(BF16), split(state)
        return plain(move, high) + plain(move, low) + both[:, :hd]

    ident = jnp.concatenate([jnp.zeros((hd, hd), F32), e64], axis=1)
    for i in range(n - 1):
        fore = [enter(i, x, h, i < me) for h, x in enumerate(fore)]
        back = [enter(n - 1 - i, x, h, n - 1 - i > me) for h, x in enumerate(back)]
    for h in range(dheads):
        o = o_loc[0, h] + o_loc[1, h] + near(r_mat[0, h], fore[h]) + near(r_mat[1, h], back[h])
        o = o * lax.rsqrt(jnp.mean(o * o, axis=-1, keepdims=True) + norm_eps) * og[...]
        lo_c = base + 3 * dw + h * hd
        gate = acc[:, lo_c : lo_c + hd].astype(BF16).astype(F32)
        joined[:, aw + h * hd : aw + (h + 1) * hd] = (o * silu(gate)).astype(BF16)

    cw = wo.shape[1]
    tr = rows // nt
    lhs = joined[...]
    for b in range(n):
        y = plain(lhs, obuf[b])
        for j in range(nt):
            part[j, :, b * cw : (b + 1) * cw] = y[j * tr : (j + 1) * tr].astype(SUM_DTYPE)
    rs_copies = [
        copy_to(
            part.at[lax.rem(t + d, nt)], rsbuf.at[d - 1], rs_s.at[d - 1], rs_r.at[d - 1],
            (me, lax.rem(t + d, nt)),
        )
        for d in range(1, nt)
    ]
    for c in rs_copies:
        c.start()
    for c in tok_copies:
        c.wait_send()
    for d in range(1, n):
        ab_copy(d).wait_send()
    wg.drain()
    ogather.drain()
    pl.when(me < n - 1)(lambda: head_to(0).wait_send())
    pl.when(me > 0)(lambda: head_to(1).wait_send())
    state_all(lambda c: c.wait_send())
    total = part[t].astype(F32)
    for d in range(1, nt):
        rs_copies[d - 1].wait_recv()
        total += rsbuf[d - 1].astype(F32)
    out[...] = total.astype(BF16)
    for c in rs_copies:
        c.wait_send()


def per_device(
    tokens, norm_gain, attn_query, attn_key, attn_value, sink_logit, delta_query, delta_key,
    delta_value, delta_gate, beta_weight, decay_weight, beta_shift, decay_log, out_gain,
    attn_out, delta_out,
):
    n, nt = lax.axis_size("sp"), lax.axis_size("tp")
    rows, width = tokens.shape
    kb = attn_query.shape[0]
    heads, kvs = attn_query.shape[1] // HEAD_DIM, attn_key.shape[1] // HEAD_DIM
    dheads = delta_query.shape[1] // HEAD_DIM
    ab = 2 * dheads
    wp = jnp.concatenate(
        [
            attn_query, attn_key, attn_value, delta_query, delta_key, delta_value, delta_gate,
        ],
        axis=1,
    )
    na = -(-2 * ab // 16) * 16
    gates = jnp.concatenate(
        [
            beta_weight.reshape(kb, ab).T, decay_weight.reshape(kb, ab).T,
            jnp.zeros((na - 2 * ab, kb), BF16),
        ],
        axis=0,
    )
    wo = jnp.concatenate([attn_out, delta_out], axis=0)
    flat = lambda a, before: jnp.pad(a, (before, na - before - a.shape[0]))
    par = jnp.stack(
        [
            flat(beta_shift.T.reshape(ab), 0),
            flat(-jnp.exp(decay_log.T.reshape(ab)) / (rows * n), ab),
            flat(sink_logit, 0),
        ],
        axis=1,
    )
    cw = wo.shape[1]
    tr = rows // nt
    hd = HEAD_DIM
    kw = kvs * hd
    dma = pltpu.SemaphoreType.DMA
    vm = pl.BlockSpec(memory_space=pltpu.VMEM)
    return pl.pallas_call(
        functools.partial(layer_kernel, n, nt, heads, kvs, dheads),
        out_shape=jax.ShapeDtypeStruct((tr, n * cw), BF16),
        in_specs=[vm] * 7,
        out_specs=vm,
        scratch_shapes=[
            pltpu.VMEM((nt, rows, width), BF16),
            pltpu.VMEM((n, rows, kb), BF16),
            pltpu.VMEM((n,) + wp.shape, BF16),
            pltpu.VMEM((n,) + wo.shape, BF16),
            pltpu.VMEM((n, na, kb), BF16),
            pltpu.VMEM((rows, wp.shape[1]), F32),
            pltpu.VMEM((rows + 2 * WINDOW, 2 * kw), BF16),
            pltpu.VMEM((2, dheads, hd, 2 * hd), BF16),
            pltpu.VMEM((n, dheads, hd, 2 * hd), BF16),
            pltpu.VMEM((2, dheads, rows, hd), F32),
            pltpu.VMEM((2, dheads, rows, hd), F32),
            pltpu.VMEM((rows, (heads + dheads) * hd), BF16),
            pltpu.VMEM((nt, tr, n * cw), SUM_DTYPE),
            pltpu.VMEM((nt - 1, tr, n * cw), SUM_DTYPE),
            dma((nt - 1,)), dma((nt,)),
            dma((3, n, PARTS)), dma((n, PARTS)),
            dma((3, n, 1)), dma((n, 1)),
            dma((n,)), dma((n,)),
            dma((2,)), dma((2,)),
            dma((n,)), dma((n,)),
            dma((nt - 1,)), dma((nt - 1,)),
        ],
        compiler_params=pltpu.CompilerParams(
            collective_id=0, has_side_effects=True, vmem_limit_bytes=48 * 1024 * 1024
        ),
    )(tokens, norm_gain.reshape(nt, width), wp, wo, gates, par, out_gain.reshape(1, hd))


def solution(mesh):
    return jax.shard_map(
        per_device,
        mesh=mesh,
        in_specs=(
            P("sp", "tp"), P(), P("sp", "tp"), P("sp", "tp"), P("sp", "tp"), P("tp"),
            P("sp", "tp"), P("sp", "tp"), P("sp", "tp"), P("sp", "tp"),
            P("sp", "tp", None), P("sp", "tp", None), P(None, "tp"), P(None, "tp"), P(),
            P("tp", "sp"), P("tp", "sp"),
        ),
        out_specs=P(("sp", "tp"), None),
        check_vma=False,
    )
```

```python
import functools

import jax
import jax.numpy as jnp
from jax import lax
from jax.experimental import pallas as pl
from jax.experimental.pallas import tpu as pltpu
from jax.sharding import PartitionSpec as P

HEAD_DIM = 64
WINDOW = 64
norm_eps = 1e-06
MESH = pl.DeviceIdType.MESH
F32 = jnp.float32
BF16 = jnp.bfloat16
SUM_DTYPE = jnp.bfloat16
PARTS = 3


def exact(a, b, dims=((1,), (0,))):
    return lax.dot_general(
        a, b, (dims, ((), ())), precision=lax.Precision.HIGHEST, preferred_element_type=F32
    )


def plain(a, b, dims=((1,), (0,))):
    return lax.dot_general(a, b, (dims, ((), ())), preferred_element_type=F32)


def split(x):
    high = x.astype(BF16)
    return high, (x - high.astype(F32)).astype(BF16)


def close(a, b, dims=((1,), (0,))):
    (ca,), (cb,) = dims
    left = jnp.concatenate([a[0], a[1], a[0]], axis=ca)
    right = jnp.concatenate([b[0], b[0], b[1]], axis=cb)
    return plain(left, right, dims)


def near(a, b, dims=((1,), (0,))):
    a, b = split(a), split(b)
    return plain(a[0], b[0], dims) + (plain(a[1], b[0], dims) + plain(a[0], b[1], dims))


def silu(x):
    return x * jax.nn.sigmoid(x)


def unit_rows(x):
    return x * lax.rsqrt(jnp.sum(x * x, axis=-1, keepdims=True) + norm_eps)


def copy_to(src, dst, send, recv, device):
    return pltpu.make_async_remote_copy(
        src_ref=src,
        dst_ref=dst,
        send_sem=send,
        recv_sem=recv,
        device_id=device,
        device_id_type=MESH,
    )


class Gather:
    def __init__(self, n, me, tp, buf, send, recv, parts):
        self.nh = n // 2
        self.me, self.tp = me, tp
        self.lo, self.hi = lax.rem(me, 2), lax.div(me, 2)
        self.buf, self.send, self.recv = buf, send, recv
        self.parts = parts
        self.size = buf.shape[2] // parts

    def copy(self, b, route, p):
        target = (self.me + 2, self.me - 2, self.hi * 2 + 1 - self.lo)[route]
        cols = pl.ds(p * self.size, self.size)
        return copy_to(
            self.buf.at[b, :, cols],
            self.buf.at[b, :, cols],
            self.send.at[route, b, p],
            self.recv.at[b, p],
            (target, self.tp),
        )

    def can(self, route):
        return self.hi < self.nh - 1 if route == 0 else self.hi > 0

    def first(self, act):
        for p in range(self.parts):
            for route in (0, 1):
                pl.when(self.can(route))(lambda p=p, route=route: act(self.copy(self.me, route, p)))
            act(self.copy(self.me, 2, p))

    def begin(self):
        self.first(lambda c: c.start())

    def sides(self, d):
        return ((0, self.hi - d, self.hi - d >= 0), (1, self.hi + d, self.hi + d < self.nh))

    def step(self, d, use=None):
        for p in range(self.parts):
            if d < self.nh:
                for route, there, ok in self.sides(d):

                    @pl.when(ok)
                    def _(route=route, there=there):
                        b = there * 2 + self.lo
                        self.copy(b, 2, p).wait_recv()
                        pl.when(self.can(route))(lambda: self.copy(b, route, p).start())
                        self.copy(b, 2, p).start()
                        if use is not None:
                            use(b, p)

            for i, (_, there, ok) in enumerate(self.sides(d - 1)):
                if d == 1 and i == 1:
                    continue

                @pl.when(ok)
                def _(there=there):
                    b = there * 2 + 1 - self.lo
                    self.copy(b, 2, p).wait_recv()
                    if use is not None:
                        use(b, p)

    def drain(self):
        self.first(lambda c: c.wait_send())
        for d in range(1, self.nh):
            for p in range(self.parts):
                for route, there, ok in self.sides(d):

                    @pl.when(ok)
                    def _(route=route, there=there):
                        b = there * 2 + self.lo
                        pl.when(self.can(route))(lambda: self.copy(b, route, p).wait_send())
                        self.copy(b, 2, p).wait_send()


def layer_kernel(
    n, nt, heads, kvs, dheads,
    tok, gain_in, aq, ak, av, dq, dk, dv, dz, ao, do, ab, par, og_in, out,
    gain, og, kvw, in_sem, tokbuf, normed, wbuf, obuf, abbuf, acc, kvbuf, st, stbuf, o_loc, r_mat, joined, part, rsbuf,
    tok_s, tok_r, w_s, w_r, o_s, o_r, ab_s, ab_r, kv_s, kv_r, st_s, st_r, rs_s, rs_r,
):
    me, t = lax.axis_index("sp"), lax.axis_index("tp")
    rows, width = tok.shape
    kb = aq.shape[0]
    hd = HEAD_DIM
    aw, kw, dw = heads * hd, kvs * hd, dheads * hd
    mine = [(tok, tokbuf.at[t])]
    at = 0
    for w in (aq, dq, dk, dv, dz):
        mine.append((w, wbuf.at[me, :, pl.ds(at, w.shape[1])]))
        at += w.shape[1]
    mine += [(ak, kvw.at[0]), (av, kvw.at[1]), (gain_in, gain), (og_in, og)]
    mine += [(ao, obuf.at[me, pl.ds(0, aw)]), (do, obuf.at[me, pl.ds(aw, dw)])]
    mine = [pltpu.make_async_copy(a, b, in_sem.at[i]) for i, (a, b) in enumerate(mine)]
    for c in mine:
        c.start()
    bar = pltpu.get_barrier_semaphore()
    for d in range(1, n):
        pl.semaphore_signal(bar, inc=1, device_id=(lax.rem(me + d, n), t), device_id_type=MESH)
    for d in range(1, nt):
        pl.semaphore_signal(bar, inc=1, device_id=(me, lax.rem(t + d, nt)), device_id_type=MESH)
    pl.semaphore_wait(bar, n - 1 + nt - 1)

    for c in mine:
        c.wait()
    wbuf[me, :, at:] = jnp.concatenate([kvw[0], kvw[1]], axis=1)
    tok_copies = [
        copy_to(tokbuf.at[t], tokbuf.at[t], tok_s.at[d - 1], tok_r.at[t], (me, lax.rem(t + d, nt)))
        for d in range(1, nt)
    ]
    for c in tok_copies:
        c.start()
    wg = Gather(n, me, t, wbuf, w_s, w_r, PARTS)
    ogather = Gather(n, me, t, obuf, o_s, o_r, 1)
    wg.begin()

    def ab_copy(d):
        p = lax.rem(me + d, n)
        return copy_to(ab, abbuf.at[me], ab_s.at[d], ab_r.at[me], (p, t))

    for d in range(1, n):
        ab_copy(d).start()
    abbuf[me] = ab[...]
    for d in range(1, nt):
        j = lax.rem(t + d, nt)
        copy_to(tokbuf.at[t], tokbuf.at[j], tok_s.at[d - 1], tok_r.at[j], (me, j)).wait_recv()
    total = jnp.zeros((rows, 1), F32)
    for j in range(nt):
        x = tokbuf[j].astype(F32)
        total += jnp.sum(x * x, axis=-1, keepdims=True)
    inverse = lax.rsqrt(total / (nt * width) + norm_eps)
    per = width // kb
    for j in range(nt):
        x = (tokbuf[j].astype(F32) * inverse * gain[:, j * width : (j + 1) * width]).astype(BF16)
        for i in range(per):
            normed[j * per + i] = x[:, i * kb : (i + 1) * kb]
    acc[...] = plain(normed[me], wbuf[me])

    half = wbuf.shape[2] // PARTS

    def use(b, p):
        cols = slice(p * half, (p + 1) * half)
        acc[:, cols] += plain(normed[b], wbuf[b, :, cols])

    for d in range(1, n // 2 + 1):
        wg.step(d, use)
    ogather.begin()

    kvbuf[WINDOW : WINDOW + rows] = acc[:, aw + 4 * dw :].astype(BF16)

    @pl.when(me == 0)
    def _():
        kvbuf[:WINDOW] = jnp.zeros((WINDOW, 2 * kw), BF16)

    @pl.when(me == n - 1)
    def _():
        kvbuf[WINDOW + rows :] = jnp.zeros((WINDOW, 2 * kw), BF16)

    base = aw
    for d in range(1, n):
        p = lax.rem(me + d, n)
        copy_to(ab, abbuf.at[p], ab_s.at[d], ab_r.at[p], (p, t)).wait_recv()
    tail = plain(abbuf[0], normed[0], ((1,), (1,)))
    for b in range(1, n):
        tail += plain(abbuf[b], normed[b], ((1,), (1,)))
    beta_t = jax.nn.sigmoid(tail + par[:, 0:1])
    soft = jnp.maximum(tail, 0.0) + jnp.log1p(jnp.exp(-jnp.abs(tail)))
    g_t = par[:, 1:2] * soft
    ri = lax.broadcasted_iota(jnp.int32, (rows, rows), 0)
    ci = lax.broadcasted_iota(jnp.int32, (rows, rows), 1)
    incl = (ri >= ci, ri <= ci)
    strict = (ri > ci, ri < ci)
    na = ab.shape[0]
    cum_t = [exact(g_t, jnp.where(m, 1.0, 0.0).astype(F32)) for m in (incl[1], incl[0])]
    stack = [beta_t] + cum_t
    if 3 * na < 128:
        stack.append(jnp.zeros((128 - 3 * na, rows), F32))
    columns = jnp.concatenate(stack, axis=0).T

    def head_to(p):
        up = copy_to(
            kvbuf.at[pl.ds(rows, WINDOW)], kvbuf.at[pl.ds(0, WINDOW)],
            kv_s.at[0], kv_r.at[0], (me + 1, t),
        )
        down = copy_to(
            kvbuf.at[pl.ds(WINDOW, WINDOW)], kvbuf.at[pl.ds(WINDOW + rows, WINDOW)],
            kv_s.at[1], kv_r.at[1], (me - 1, t),
        )
        return (up, down)[p]

    pl.when(me < n - 1)(lambda: head_to(0).start())
    pl.when(me > 0)(lambda: head_to(1).start())

    chains = []
    qs = []
    for h in range(dheads):
        def cols(i):
            lo_c = base + i * dw + h * hd
            return acc[:, lo_c : lo_c + hd].astype(BF16).astype(F32)

        q = unit_rows(silu(cols(0))) * hd ** (-0.5)
        k = unit_rows(silu(cols(1)))
        v = silu(cols(2))
        kk = near(k, k, ((1,), (1,)))
        qk = near(q, k, ((1,), (1,)))
        for r in range(2):
            c = h * 2 + r
            lane = 2 * dheads + c
            at = (1 + r) * na + lane
            gcol = columns[:, at : at + 1]
            grow = cum_t[r][lane : lane + 1, :]
            beta = columns[:, c : c + 1]
            decay = jnp.where(incl[r], jnp.exp(jnp.minimum(gcol - grow, 0.0)), 0.0)
            a = jnp.where(strict[r], beta * kk * decay, 0.0)
            eg = jnp.exp(gcol)
            last = gcol[rows - 1 : rows, :] if r == 0 else gcol[0:1, :]
            chains.append(
                dict(
                    r=r, h=h, a=a, rhs=jnp.concatenate([beta * v, beta * k * eg], axis=1),
                    pm=qk * decay, qe=q * eg, kd=(k * jnp.exp(last - gcol)).T, last=last,
                )
            )
    size = 1
    while (1 << size) <= rows:
        size += 1
    levels = size - 1
    eye = jnp.where(ri == ci, 1.0, 0.0).astype(F32)
    xor = ri ^ ci
    inv = [eye - jnp.where(xor == 1, ch["a"], 0.0) for ch in chains]
    pairs = [split(ch["a"]) for ch in chains]
    ogather.step(1)
    for lv in range(1, levels):
        m = jnp.where((xor >> lv) == 1, 1.0, 0.0).astype(BF16)
        xs = [split(x) for x in inv]
        left = [close(x, (m * a[0], m * a[1])) for x, a in zip(xs, pairs)]
        inv = [x - close(split(y), z) for x, y, z in zip(inv, left, xs)]
    sols = [split(close(split(x), split(ch["rhs"]))) for x, ch in zip(inv, chains)]
    outs = [close(split(ch["kd"]), s) for ch, s in zip(chains, sols)]
    e64 = jnp.where(
        lax.broadcasted_iota(jnp.int32, (hd, hd), 0)
        == lax.broadcasted_iota(jnp.int32, (hd, hd), 1), 1.0, 0.0,
    ).astype(F32)
    for ch, s in zip(chains, outs):
        full = jnp.concatenate([s[:, :hd], jnp.exp(ch["last"]) * e64 - s[:, hd:]], axis=1)
        st[ch["r"], ch["h"]] = full.astype(BF16)
    def state_copy(r, p):
        return copy_to(st.at[r], stbuf.at[me], st_s.at[p], st_r.at[me], (p, t))

    def state_all(act):
        for d in range(n - 1, 0, -1):
            pl.when(me + d < n)(lambda d=d: act(state_copy(0, me + d)))
            pl.when(me - d >= 0)(lambda d=d: act(state_copy(1, me - d)))

    state_all(lambda c: c.start())
    inner = [close(split(ch["pm"]), s) for ch, s in zip(chains, sols)]
    for ch, s in zip(chains, inner):
        o_loc[ch["r"], ch["h"]] = s[:, :hd]
        r_mat[ch["r"], ch["h"]] = ch["qe"] - s[:, hd:]


    ogather.step(2)

    pl.when(me > 0)(lambda: head_to(0).wait_recv())
    pl.when(me < n - 1)(lambda: head_to(1).wait_recv())
    span = rows + 2 * WINDOW
    qi = lax.broadcasted_iota(jnp.int32, (rows, span), 0)
    kj = lax.broadcasted_iota(jnp.int32, (rows, span), 1) - WINDOW
    pos = kj + me * rows
    allowed = (jnp.abs(qi - kj) <= WINDOW) & (pos >= 0) & (pos < n * rows)
    for h in range(heads):
        g = h // (heads // kvs)
        q = acc[:, h * hd : (h + 1) * hd].astype(BF16)
        s = plain(q, kvbuf[:, g * hd : (g + 1) * hd], ((1,), (1,))) * hd ** (-0.5)
        s = jnp.where(allowed, s, -jnp.inf)
        sink = par[h : h + 1, 2:3]
        m = jnp.maximum(jnp.max(s, axis=-1, keepdims=True), sink)
        e = jnp.exp(s - m)
        p = e / (jnp.sum(e, axis=-1, keepdims=True) + jnp.exp(sink - m))
        o = plain(p.astype(BF16), kvbuf[:, kw + g * hd : kw + (g + 1) * hd])
        joined[:, h * hd : (h + 1) * hd] = o.astype(BF16)
    for d in range(3, n // 2):
        ogather.step(d)

    for i in range(n):

        @pl.when(me != i)
        def _(i=i):
            copy_to(st.at[0], stbuf.at[i], st_s.at[i], st_r.at[i], (me, t)).wait_recv()

    fore = [jnp.zeros((hd, hd), F32)] * dheads
    back = [jnp.zeros((hd, hd), F32)] * dheads

    def enter(i, state, h, ok):
        both = jnp.where(ok, stbuf[i, h].astype(F32), ident)
        move, (high, low) = both[:, hd:].astype(BF16), split(state)
        return plain(move, high) + plain(move, low) + both[:, :hd]

    ident = jnp.concatenate([jnp.zeros((hd, hd), F32), e64], axis=1)
    for i in range(n - 1):
        fore = [enter(i, x, h, i < me) for h, x in enumerate(fore)]
        back = [enter(n - 1 - i, x, h, n - 1 - i > me) for h, x in enumerate(back)]
    if n // 2 > 2:
        ogather.step(n // 2)
    for h in range(dheads):
        o = o_loc[0, h] + o_loc[1, h] + near(r_mat[0, h], fore[h]) + near(r_mat[1, h], back[h])
        o = o * lax.rsqrt(jnp.mean(o * o, axis=-1, keepdims=True) + norm_eps) * og[...]
        lo_c = base + 3 * dw + h * hd
        gate = acc[:, lo_c : lo_c + hd].astype(BF16).astype(F32)
        joined[:, aw + h * hd : aw + (h + 1) * hd] = (o * silu(gate)).astype(BF16)

    cw = ao.shape[1]
    tr = rows // nt
    lhs = joined[...]
    for b in range(n):
        y = plain(lhs, obuf[b])
        for j in range(nt):
            part[j, :, b * cw : (b + 1) * cw] = y[j * tr : (j + 1) * tr].astype(SUM_DTYPE)
    rs_copies = [
        copy_to(
            part.at[lax.rem(t + d, nt)], rsbuf.at[d - 1], rs_s.at[d - 1], rs_r.at[d - 1],
            (me, lax.rem(t + d, nt)),
        )
        for d in range(1, nt)
    ]
    for c in rs_copies:
        c.start()
    for c in tok_copies:
        c.wait_send()
    for d in range(1, n):
        ab_copy(d).wait_send()
    wg.drain()
    ogather.drain()
    pl.when(me < n - 1)(lambda: head_to(0).wait_send())
    pl.when(me > 0)(lambda: head_to(1).wait_send())
    state_all(lambda c: c.wait_send())
    total = part[t].astype(F32)
    for d in range(1, nt):
        rs_copies[d - 1].wait_recv()
        total += rsbuf[d - 1].astype(F32)
    out[...] = total.astype(BF16)
    for c in rs_copies:
        c.wait_send()


def per_device(
    tokens, norm_gain, attn_query, attn_key, attn_value, sink_logit, delta_query, delta_key,
    delta_value, delta_gate, beta_weight, decay_weight, beta_shift, decay_log, out_gain,
    attn_out, delta_out,
):
    n, nt = lax.axis_size("sp"), lax.axis_size("tp")
    rows, width = tokens.shape
    kb = attn_query.shape[0]
    heads, kvs = attn_query.shape[1] // HEAD_DIM, attn_key.shape[1] // HEAD_DIM
    dheads = delta_query.shape[1] // HEAD_DIM
    ab = 2 * dheads
    wide = (2 * kvs + heads + 4 * dheads) * HEAD_DIM
    na = -(-2 * ab // 16) * 16
    gates = jnp.concatenate(
        [
            beta_weight.reshape(kb, ab).T, decay_weight.reshape(kb, ab).T,
            jnp.zeros((na - 2 * ab, kb), BF16),
        ],
        axis=0,
    )
    flat = lambda a, before: jnp.pad(a, (before, na - before - a.shape[0]))
    par = jnp.stack(
        [
            flat(beta_shift.T.reshape(ab), 0),
            flat(-jnp.exp(decay_log.T.reshape(ab)) / (rows * n), ab),
            flat(sink_logit, 0),
        ],
        axis=1,
    )
    cw = attn_out.shape[1]
    tr = rows // nt
    hd = HEAD_DIM
    kw = kvs * hd
    dma = pltpu.SemaphoreType.DMA
    vm = pl.BlockSpec(memory_space=pltpu.VMEM)
    hbm = pl.BlockSpec(memory_space=pl.ANY)
    return pl.pallas_call(
        functools.partial(layer_kernel, n, nt, heads, kvs, dheads),
        out_shape=jax.ShapeDtypeStruct((tr, n * cw), BF16),
        in_specs=[hbm] * 11 + [vm] * 2 + [hbm],
        out_specs=vm,
        scratch_shapes=[
            pltpu.VMEM((1, nt * width), F32),
            pltpu.VMEM((1, hd), F32),
            pltpu.VMEM((2, kb, kw), BF16),
            dma((12,)),
            pltpu.VMEM((nt, rows, width), BF16),
            pltpu.VMEM((n, rows, kb), BF16),
            pltpu.VMEM((n, kb, wide), BF16),
            pltpu.VMEM((n, (heads + dheads) * hd, cw), BF16),
            pltpu.VMEM((n, na, kb), BF16),
            pltpu.VMEM((rows, wide), F32),
            pltpu.VMEM((rows + 2 * WINDOW, 2 * kw), BF16),
            pltpu.VMEM((2, dheads, hd, 2 * hd), BF16),
            pltpu.VMEM((n, dheads, hd, 2 * hd), BF16),
            pltpu.VMEM((2, dheads, rows, hd), F32),
            pltpu.VMEM((2, dheads, rows, hd), F32),
            pltpu.VMEM((rows, (heads + dheads) * hd), BF16),
            pltpu.VMEM((nt, tr, n * cw), SUM_DTYPE),
            pltpu.VMEM((nt - 1, tr, n * cw), SUM_DTYPE),
            dma((nt - 1,)), dma((nt,)),
            dma((3, n, PARTS)), dma((n, PARTS)),
            dma((3, n, 1)), dma((n, 1)),
            dma((n,)), dma((n,)),
            dma((2,)), dma((2,)),
            dma((n,)), dma((n,)),
            dma((nt - 1,)), dma((nt - 1,)),
        ],
        compiler_params=pltpu.CompilerParams(
            collective_id=0, has_side_effects=True, vmem_limit_bytes=48 * 1024 * 1024
        ),
    )(
        tokens, norm_gain.reshape(1, nt * width), attn_query, attn_key, attn_value, delta_query,
        delta_key, delta_value, delta_gate, attn_out, delta_out, gates, par,
        out_gain.reshape(1, hd),
    )


def solution(mesh):
    return jax.shard_map(
        per_device,
        mesh=mesh,
        in_specs=(
            P("sp", "tp"), P(), P("sp", "tp"), P("sp", "tp"), P("sp", "tp"), P("tp"),
            P("sp", "tp"), P("sp", "tp"), P("sp", "tp"), P("sp", "tp"),
            P("sp", "tp", None), P("sp", "tp", None), P(None, "tp"), P(None, "tp"), P(),
            P("tp", "sp"), P("tp", "sp"),
        ),
        out_specs=P(("sp", "tp"), None),
        check_vma=False,
    )
```

```python
import functools

import jax
import jax.numpy as jnp
from jax import lax
from jax.experimental import pallas as pl
from jax.experimental.pallas import tpu as pltpu
from jax.sharding import PartitionSpec as P

HEAD_DIM = 64
WINDOW = 64
norm_eps = 1e-06
MESH = pl.DeviceIdType.MESH
F32 = jnp.float32
BF16 = jnp.bfloat16
SUM_DTYPE = jnp.bfloat16
PARTS = 3


def exact(a, b, dims=((1,), (0,))):
    return lax.dot_general(
        a, b, (dims, ((), ())), precision=lax.Precision.HIGHEST, preferred_element_type=F32
    )


def plain(a, b, dims=((1,), (0,))):
    return lax.dot_general(a, b, (dims, ((), ())), preferred_element_type=F32)


def split(x):
    high = x.astype(BF16)
    return high, (x - high.astype(F32)).astype(BF16)


def close(a, b, dims=((1,), (0,))):
    (ca,), (cb,) = dims
    left = jnp.concatenate([a[0], a[1], a[0]], axis=ca)
    right = jnp.concatenate([b[0], b[0], b[1]], axis=cb)
    return plain(left, right, dims)


def near(a, b, dims=((1,), (0,))):
    a, b = split(a), split(b)
    return plain(a[0], b[0], dims) + (plain(a[1], b[0], dims) + plain(a[0], b[1], dims))


def silu(x):
    return x * jax.nn.sigmoid(x)


def unit_rows(x):
    return x * lax.rsqrt(jnp.sum(x * x, axis=-1, keepdims=True) + norm_eps)


def copy_to(src, dst, send, recv, device):
    return pltpu.make_async_remote_copy(
        src_ref=src,
        dst_ref=dst,
        send_sem=send,
        recv_sem=recv,
        device_id=device,
        device_id_type=MESH,
    )


class Gather:
    def __init__(self, n, me, tp, buf, send, recv, parts):
        self.nh = n // 2
        self.me, self.tp = me, tp
        self.lo, self.hi = lax.rem(me, 2), lax.div(me, 2)
        self.buf, self.send, self.recv = buf, send, recv
        self.parts = parts
        self.size = buf.shape[2] // parts

    def copy(self, b, route, p):
        target = (self.me + 2, self.me - 2, self.hi * 2 + 1 - self.lo)[route]
        cols = pl.ds(p * self.size, self.size)
        return copy_to(
            self.buf.at[b, :, cols],
            self.buf.at[b, :, cols],
            self.send.at[route, b, p],
            self.recv.at[b, p],
            (target, self.tp),
        )

    def can(self, route):
        return self.hi < self.nh - 1 if route == 0 else self.hi > 0

    def first(self, act):
        for p in range(self.parts):
            for route in (0, 1):
                pl.when(self.can(route))(lambda p=p, route=route: act(self.copy(self.me, route, p)))
            act(self.copy(self.me, 2, p))

    def begin(self):
        self.first(lambda c: c.start())

    def sides(self, d):
        return ((0, self.hi - d, self.hi - d >= 0), (1, self.hi + d, self.hi + d < self.nh))

    def step(self, d, use=None):
        for p in range(self.parts):
            if d < self.nh:
                for route, there, ok in self.sides(d):

                    @pl.when(ok)
                    def _(route=route, there=there):
                        b = there * 2 + self.lo
                        self.copy(b, 2, p).wait_recv()
                        pl.when(self.can(route))(lambda: self.copy(b, route, p).start())
                        self.copy(b, 2, p).start()
                        if use is not None:
                            use(b, p)

            for i, (_, there, ok) in enumerate(self.sides(d - 1)):
                if d == 1 and i == 1:
                    continue

                @pl.when(ok)
                def _(there=there):
                    b = there * 2 + 1 - self.lo
                    self.copy(b, 2, p).wait_recv()
                    if use is not None:
                        use(b, p)

    def drain(self):
        self.first(lambda c: c.wait_send())
        for d in range(1, self.nh):
            for p in range(self.parts):
                for route, there, ok in self.sides(d):

                    @pl.when(ok)
                    def _(route=route, there=there):
                        b = there * 2 + self.lo
                        pl.when(self.can(route))(lambda: self.copy(b, route, p).wait_send())
                        self.copy(b, 2, p).wait_send()


def layer_kernel(
    n, nt, heads, kvs, dheads,
    tok, gain_in, aq, ak, av, dq, dk, dv, dz, ao, do, ab, par, og_in, out,
    gain, og, kvw, in_sem, tokbuf, normed, wbuf, obuf, abbuf, acc, kvbuf, st, stbuf, o_loc, r_mat, joined, part, rsbuf,
    tok_s, tok_r, w_s, w_r, o_s, o_r, ab_s, ab_r, kv_s, kv_r, st_s, st_r, rs_s, rs_r,
):
    me, t = lax.axis_index("sp"), lax.axis_index("tp")
    rows, width = tok.shape
    kb = aq.shape[0]
    hd = HEAD_DIM
    aw, kw, dw = heads * hd, kvs * hd, dheads * hd
    mine = [(tok, tokbuf.at[t])]
    at = 0
    for w in (aq, dq, dk, dv, dz):
        mine.append((w, wbuf.at[me, :, pl.ds(at, w.shape[1])]))
        at += w.shape[1]
    mine += [(ak, kvw.at[pl.ds(0, kw)]), (av, kvw.at[pl.ds(kw, kw)]), (gain_in, gain), (og_in, og)]
    mine += [(ao, obuf.at[me, pl.ds(0, aw)]), (do, obuf.at[me, pl.ds(aw, dw)])]
    mine = [pltpu.make_async_copy(a, b, in_sem.at[i]) for i, (a, b) in enumerate(mine)]
    for c in mine:
        c.start()
    bar = pltpu.get_barrier_semaphore()
    for d in range(1, n):
        pl.semaphore_signal(bar, inc=1, device_id=(lax.rem(me + d, n), t), device_id_type=MESH)
    for d in range(1, nt):
        pl.semaphore_signal(bar, inc=1, device_id=(me, lax.rem(t + d, nt)), device_id_type=MESH)
    pl.semaphore_wait(bar, n - 1 + nt - 1)

    for c in mine:
        c.wait()
    wbuf[me, :, at:] = kvw[...].T
    tok_copies = [
        copy_to(tokbuf.at[t], tokbuf.at[t], tok_s.at[d - 1], tok_r.at[t], (me, lax.rem(t + d, nt)))
        for d in range(1, nt)
    ]
    for c in tok_copies:
        c.start()
    wg = Gather(n, me, t, wbuf, w_s, w_r, PARTS)
    ogather = Gather(n, me, t, obuf, o_s, o_r, 1)
    wg.begin()

    def ab_copy(d):
        p = lax.rem(me + d, n)
        return copy_to(ab, abbuf.at[me], ab_s.at[d], ab_r.at[me], (p, t))

    for d in range(1, n):
        ab_copy(d).start()
    abbuf[me] = ab[...]
    for d in range(1, nt):
        j = lax.rem(t + d, nt)
        copy_to(tokbuf.at[t], tokbuf.at[j], tok_s.at[d - 1], tok_r.at[j], (me, j)).wait_recv()
    total = jnp.zeros((rows, 1), F32)
    for j in range(nt):
        x = tokbuf[j].astype(F32)
        total += jnp.sum(x * x, axis=-1, keepdims=True)
    inverse = lax.rsqrt(total / (nt * width) + norm_eps)
    per = width // kb
    for j in range(nt):
        x = (tokbuf[j].astype(F32) * inverse * gain[:, j * width : (j + 1) * width]).astype(BF16)
        for i in range(per):
            normed[j * per + i] = x[:, i * kb : (i + 1) * kb]
    acc[...] = plain(normed[me], wbuf[me])

    half = wbuf.shape[2] // PARTS

    def use(b, p):
        cols = slice(p * half, (p + 1) * half)
        acc[:, cols] += plain(normed[b], wbuf[b, :, cols])

    for d in range(1, n // 2 + 1):
        wg.step(d, use)
    ogather.begin()

    kvbuf[WINDOW : WINDOW + rows] = acc[:, aw + 4 * dw :].astype(BF16)

    @pl.when(me == 0)
    def _():
        kvbuf[:WINDOW] = jnp.zeros((WINDOW, 2 * kw), BF16)

    @pl.when(me == n - 1)
    def _():
        kvbuf[WINDOW + rows :] = jnp.zeros((WINDOW, 2 * kw), BF16)

    base = aw
    for d in range(1, n):
        p = lax.rem(me + d, n)
        copy_to(ab, abbuf.at[p], ab_s.at[d], ab_r.at[p], (p, t)).wait_recv()
    tail = plain(abbuf[0], normed[0], ((1,), (1,)))
    for b in range(1, n):
        tail += plain(abbuf[b], normed[b], ((1,), (1,)))
    beta_t = jax.nn.sigmoid(tail + par[:, 0:1])
    soft = jnp.maximum(tail, 0.0) + jnp.log1p(jnp.exp(-jnp.abs(tail)))
    g_t = par[:, 1:2] * soft
    ri = lax.broadcasted_iota(jnp.int32, (rows, rows), 0)
    ci = lax.broadcasted_iota(jnp.int32, (rows, rows), 1)
    incl = (ri >= ci, ri <= ci)
    strict = (ri > ci, ri < ci)
    na = ab.shape[0]
    cum_t = [exact(g_t, jnp.where(m, 1.0, 0.0).astype(F32)) for m in (incl[1], incl[0])]
    stack = [beta_t] + cum_t
    if 3 * na < 128:
        stack.append(jnp.zeros((128 - 3 * na, rows), F32))
    columns = jnp.concatenate(stack, axis=0).T

    def head_to(p):
        up = copy_to(
            kvbuf.at[pl.ds(rows, WINDOW)], kvbuf.at[pl.ds(0, WINDOW)],
            kv_s.at[0], kv_r.at[0], (me + 1, t),
        )
        down = copy_to(
            kvbuf.at[pl.ds(WINDOW, WINDOW)], kvbuf.at[pl.ds(WINDOW + rows, WINDOW)],
            kv_s.at[1], kv_r.at[1], (me - 1, t),
        )
        return (up, down)[p]

    pl.when(me < n - 1)(lambda: head_to(0).start())
    pl.when(me > 0)(lambda: head_to(1).start())

    chains = []
    qs = []
    for h in range(dheads):
        def cols(i):
            lo_c = base + i * dw + h * hd
            return acc[:, lo_c : lo_c + hd].astype(BF16).astype(F32)

        q = unit_rows(silu(cols(0))) * hd ** (-0.5)
        k = unit_rows(silu(cols(1)))
        v = silu(cols(2))
        kk = near(k, k, ((1,), (1,)))
        qk = near(q, k, ((1,), (1,)))
        for r in range(2):
            c = h * 2 + r
            lane = 2 * dheads + c
            at = (1 + r) * na + lane
            gcol = columns[:, at : at + 1]
            grow = cum_t[r][lane : lane + 1, :]
            beta = columns[:, c : c + 1]
            decay = jnp.where(incl[r], jnp.exp(jnp.minimum(gcol - grow, 0.0)), 0.0)
            a = jnp.where(strict[r], beta * kk * decay, 0.0)
            eg = jnp.exp(gcol)
            last = gcol[rows - 1 : rows, :] if r == 0 else gcol[0:1, :]
            chains.append(
                dict(
                    r=r, h=h, a=a, rhs=jnp.concatenate([beta * v, beta * k * eg], axis=1),
                    pm=qk * decay, qe=q * eg, kd=(k * jnp.exp(last - gcol)).T, last=last,
                )
            )
    size = 1
    while (1 << size) <= rows:
        size += 1
    levels = size - 1
    eye = jnp.where(ri == ci, 1.0, 0.0).astype(F32)
    xor = ri ^ ci
    inv = [eye - jnp.where(xor == 1, ch["a"], 0.0) for ch in chains]
    pairs = [split(ch["a"]) for ch in chains]
    ogather.step(1)
    for lv in range(1, levels):
        m = jnp.where((xor >> lv) == 1, 1.0, 0.0).astype(BF16)
        xs = [split(x) for x in inv]
        left = [close(x, (m * a[0], m * a[1])) for x, a in zip(xs, pairs)]
        inv = [x - close(split(y), z) for x, y, z in zip(inv, left, xs)]
    sols = [split(close(split(x), split(ch["rhs"]))) for x, ch in zip(inv, chains)]
    outs = [close(split(ch["kd"]), s) for ch, s in zip(chains, sols)]
    e64 = jnp.where(
        lax.broadcasted_iota(jnp.int32, (hd, hd), 0)
        == lax.broadcasted_iota(jnp.int32, (hd, hd), 1), 1.0, 0.0,
    ).astype(F32)
    for ch, s in zip(chains, outs):
        full = jnp.concatenate([s[:, :hd], jnp.exp(ch["last"]) * e64 - s[:, hd:]], axis=1)
        st[ch["r"], ch["h"]] = full.astype(BF16)
    def state_copy(r, p):
        return copy_to(st.at[r], stbuf.at[me], st_s.at[p], st_r.at[me], (p, t))

    def state_all(act):
        for d in range(n - 1, 0, -1):
            pl.when(me + d < n)(lambda d=d: act(state_copy(0, me + d)))
            pl.when(me - d >= 0)(lambda d=d: act(state_copy(1, me - d)))

    state_all(lambda c: c.start())
    inner = [close(split(ch["pm"]), s) for ch, s in zip(chains, sols)]
    for ch, s in zip(chains, inner):
        o_loc[ch["r"], ch["h"]] = s[:, :hd]
        r_mat[ch["r"], ch["h"]] = ch["qe"] - s[:, hd:]


    ogather.step(2)

    pl.when(me > 0)(lambda: head_to(0).wait_recv())
    pl.when(me < n - 1)(lambda: head_to(1).wait_recv())
    span = rows + 2 * WINDOW
    qi = lax.broadcasted_iota(jnp.int32, (rows, span), 0)
    kj = lax.broadcasted_iota(jnp.int32, (rows, span), 1) - WINDOW
    pos = kj + me * rows
    allowed = (jnp.abs(qi - kj) <= WINDOW) & (pos >= 0) & (pos < n * rows)
    for h in range(heads):
        g = h // (heads // kvs)
        q = acc[:, h * hd : (h + 1) * hd].astype(BF16)
        s = plain(q, kvbuf[:, g * hd : (g + 1) * hd], ((1,), (1,))) * hd ** (-0.5)
        s = jnp.where(allowed, s, -jnp.inf)
        sink = par[h : h + 1, 2:3]
        m = jnp.maximum(jnp.max(s, axis=-1, keepdims=True), sink)
        e = jnp.exp(s - m)
        p = e / (jnp.sum(e, axis=-1, keepdims=True) + jnp.exp(sink - m))
        o = plain(p.astype(BF16), kvbuf[:, kw + g * hd : kw + (g + 1) * hd])
        joined[:, h * hd : (h + 1) * hd] = o.astype(BF16)
    for d in range(3, n // 2):
        ogather.step(d)

    for i in range(n):

        @pl.when(me != i)
        def _(i=i):
            copy_to(st.at[0], stbuf.at[i], st_s.at[i], st_r.at[i], (me, t)).wait_recv()

    fore = [jnp.zeros((hd, hd), F32)] * dheads
    back = [jnp.zeros((hd, hd), F32)] * dheads

    def enter(i, state, h, ok):
        both = jnp.where(ok, stbuf[i, h].astype(F32), ident)
        move, (high, low) = both[:, hd:].astype(BF16), split(state)
        return plain(move, high) + plain(move, low) + both[:, :hd]

    ident = jnp.concatenate([jnp.zeros((hd, hd), F32), e64], axis=1)
    for i in range(n - 1):
        fore = [enter(i, x, h, i < me) for h, x in enumerate(fore)]
        back = [enter(n - 1 - i, x, h, n - 1 - i > me) for h, x in enumerate(back)]
    if n // 2 > 2:
        ogather.step(n // 2)
    for h in range(dheads):
        o = o_loc[0, h] + o_loc[1, h] + near(r_mat[0, h], fore[h]) + near(r_mat[1, h], back[h])
        o = o * lax.rsqrt(jnp.mean(o * o, axis=-1, keepdims=True) + norm_eps) * og[...]
        lo_c = base + 3 * dw + h * hd
        gate = acc[:, lo_c : lo_c + hd].astype(BF16).astype(F32)
        joined[:, aw + h * hd : aw + (h + 1) * hd] = (o * silu(gate)).astype(BF16)

    cw = ao.shape[1]
    tr = rows // nt
    lhs = joined[...]
    for b in range(n):
        y = plain(lhs, obuf[b])
        for j in range(nt):
            part[j, :, b * cw : (b + 1) * cw] = y[j * tr : (j + 1) * tr].astype(SUM_DTYPE)
    rs_copies = [
        copy_to(
            part.at[lax.rem(t + d, nt)], rsbuf.at[d - 1], rs_s.at[d - 1], rs_r.at[d - 1],
            (me, lax.rem(t + d, nt)),
        )
        for d in range(1, nt)
    ]
    for c in rs_copies:
        c.start()
    own = joined[pl.ds(pl.multiple_of(t * tr, tr), tr)]
    for c in tok_copies:
        c.wait_send()
    for d in range(1, n):
        ab_copy(d).wait_send()
    wg.drain()
    ogather.drain()
    pl.when(me < n - 1)(lambda: head_to(0).wait_send())
    pl.when(me > 0)(lambda: head_to(1).wait_send())
    state_all(lambda c: c.wait_send())
    total = jnp.concatenate([plain(own, obuf[b]) for b in range(n)], axis=1)
    for d in range(1, nt):
        rs_copies[d - 1].wait_recv()
        total += rsbuf[d - 1].astype(F32)
    out[...] = total.astype(BF16)
    for c in rs_copies:
        c.wait_send()


def per_device(
    tokens, norm_gain, attn_query, attn_key, attn_value, sink_logit, delta_query, delta_key,
    delta_value, delta_gate, beta_weight, decay_weight, beta_shift, decay_log, out_gain,
    attn_out, delta_out,
):
    n, nt = lax.axis_size("sp"), lax.axis_size("tp")
    rows, width = tokens.shape
    kb = attn_query.shape[0]
    heads, kvs = attn_query.shape[1] // HEAD_DIM, attn_key.shape[1] // HEAD_DIM
    dheads = delta_query.shape[1] // HEAD_DIM
    ab = 2 * dheads
    wide = (2 * kvs + heads + 4 * dheads) * HEAD_DIM
    na = -(-2 * ab // 16) * 16
    gates = jnp.concatenate(
        [
            beta_weight.reshape(kb, ab).T, decay_weight.reshape(kb, ab).T,
            jnp.zeros((na - 2 * ab, kb), BF16),
        ],
        axis=0,
    )
    flat = lambda a, before: jnp.pad(a, (before, na - before - a.shape[0]))
    par = jnp.stack(
        [
            flat(beta_shift.T.reshape(ab), 0),
            flat(-jnp.exp(decay_log.T.reshape(ab)) / (rows * n), ab),
            flat(sink_logit, 0),
        ],
        axis=1,
    )
    cw = attn_out.shape[1]
    tr = rows // nt
    hd = HEAD_DIM
    kw = kvs * hd
    dma = pltpu.SemaphoreType.DMA
    vm = pl.BlockSpec(memory_space=pltpu.VMEM)
    hbm = pl.BlockSpec(memory_space=pltpu.HBM)
    return pl.pallas_call(
        functools.partial(layer_kernel, n, nt, heads, kvs, dheads),
        out_shape=jax.ShapeDtypeStruct((tr, n * cw), BF16),
        in_specs=[hbm] * 11 + [vm] * 2 + [hbm],
        out_specs=vm,
        scratch_shapes=[
            pltpu.VMEM((1, nt * width), F32),
            pltpu.VMEM((1, hd), F32),
            pltpu.VMEM((2 * kw, kb), BF16),
            dma((12,)),
            pltpu.VMEM((nt, rows, width), BF16),
            pltpu.VMEM((n, rows, kb), BF16),
            pltpu.VMEM((n, kb, wide), BF16),
            pltpu.VMEM((n, (heads + dheads) * hd, cw), BF16),
            pltpu.VMEM((n, na, kb), BF16),
            pltpu.VMEM((rows, wide), F32),
            pltpu.VMEM((rows + 2 * WINDOW, 2 * kw), BF16),
            pltpu.VMEM((2, dheads, hd, 2 * hd), BF16),
            pltpu.VMEM((n, dheads, hd, 2 * hd), BF16),
            pltpu.VMEM((2, dheads, rows, hd), F32),
            pltpu.VMEM((2, dheads, rows, hd), F32),
            pltpu.VMEM((rows, (heads + dheads) * hd), BF16),
            pltpu.VMEM((nt, tr, n * cw), SUM_DTYPE),
            pltpu.VMEM((nt - 1, tr, n * cw), SUM_DTYPE),
            dma((nt - 1,)), dma((nt,)),
            dma((3, n, PARTS)), dma((n, PARTS)),
            dma((3, n, 1)), dma((n, 1)),
            dma((n,)), dma((n,)),
            dma((2,)), dma((2,)),
            dma((n,)), dma((n,)),
            dma((nt - 1,)), dma((nt - 1,)),
        ],
        compiler_params=pltpu.CompilerParams(
            collective_id=0, has_side_effects=True, vmem_limit_bytes=48 * 1024 * 1024
        ),
    )(
        tokens, norm_gain.reshape(1, nt * width), attn_query, attn_key.T, attn_value.T, delta_query,
        delta_key, delta_value, delta_gate, attn_out, delta_out, gates, par,
        out_gain.reshape(1, hd),
    )


def solution(mesh):
    return jax.shard_map(
        per_device,
        mesh=mesh,
        in_specs=(
            P("sp", "tp"), P(), P("sp", "tp"), P("sp", "tp"), P("sp", "tp"), P("tp"),
            P("sp", "tp"), P("sp", "tp"), P("sp", "tp"), P("sp", "tp"),
            P("sp", "tp", None), P("sp", "tp", None), P(None, "tp"), P(None, "tp"), P(),
            P("tp", "sp"), P("tp", "sp"),
        ),
        out_specs=P(("sp", "tp"), None),
        check_vma=False,
    )
```

```python
import functools

import jax
import jax.numpy as jnp
from jax import lax
from jax.experimental import pallas as pl
from jax.experimental.pallas import tpu as pltpu
from jax.sharding import PartitionSpec as P

HEAD_DIM = 64
WINDOW = 64
norm_eps = 1e-06
MESH = pl.DeviceIdType.MESH
F32 = jnp.float32
BF16 = jnp.bfloat16
SUM_DTYPE = jnp.bfloat16
PARTS = 3


def exact(a, b, dims=((1,), (0,))):
    return lax.dot_general(
        a, b, (dims, ((), ())), precision=lax.Precision.HIGHEST, preferred_element_type=F32
    )


def plain(a, b, dims=((1,), (0,))):
    return lax.dot_general(a, b, (dims, ((), ())), preferred_element_type=F32)


def split(x):
    high = x.astype(BF16)
    return high, (x - high.astype(F32)).astype(BF16)


def close(a, b, dims=((1,), (0,))):
    (ca,), (cb,) = dims
    left = jnp.concatenate([a[0], a[1], a[0]], axis=ca)
    right = jnp.concatenate([b[0], b[0], b[1]], axis=cb)
    return plain(left, right, dims)


def near(a, b, dims=((1,), (0,))):
    a, b = split(a), split(b)
    return plain(a[0], b[0], dims) + (plain(a[1], b[0], dims) + plain(a[0], b[1], dims))


def silu(x):
    return x * jax.nn.sigmoid(x)


def unit_rows(x):
    return x * lax.rsqrt(jnp.sum(x * x, axis=-1, keepdims=True) + norm_eps)


def copy_to(src, dst, send, recv, device):
    return pltpu.make_async_remote_copy(
        src_ref=src,
        dst_ref=dst,
        send_sem=send,
        recv_sem=recv,
        device_id=device,
        device_id_type=MESH,
    )


class Gather:
    def __init__(self, n, me, tp, buf, send, recv, parts):
        self.nh = n // 2
        self.me, self.tp = me, tp
        self.lo, self.hi = lax.rem(me, 2), lax.div(me, 2)
        self.buf, self.send, self.recv = buf, send, recv
        self.parts = parts
        self.size = buf.shape[2] // parts

    def copy(self, b, route, p):
        target = (self.me + 2, self.me - 2, self.hi * 2 + 1 - self.lo)[route]
        cols = pl.ds(p * self.size, self.size)
        return copy_to(
            self.buf.at[b, :, cols],
            self.buf.at[b, :, cols],
            self.send.at[route, b, p],
            self.recv.at[b, p],
            (target, self.tp),
        )

    def can(self, route):
        return self.hi < self.nh - 1 if route == 0 else self.hi > 0

    def first(self, act):
        for p in range(self.parts):
            for route in (0, 1):
                pl.when(self.can(route))(lambda p=p, route=route: act(self.copy(self.me, route, p)))
            act(self.copy(self.me, 2, p))

    def begin(self):
        self.first(lambda c: c.start())

    def sides(self, d):
        return ((0, self.hi - d, self.hi - d >= 0), (1, self.hi + d, self.hi + d < self.nh))

    def step(self, d, use=None):
        for p in range(self.parts):
            if d < self.nh:
                for route, there, ok in self.sides(d):

                    @pl.when(ok)
                    def _(route=route, there=there):
                        b = there * 2 + self.lo
                        self.copy(b, 2, p).wait_recv()
                        pl.when(self.can(route))(lambda: self.copy(b, route, p).start())
                        self.copy(b, 2, p).start()
                        if use is not None:
                            use(b, p)

            for i, (_, there, ok) in enumerate(self.sides(d - 1)):
                if d == 1 and i == 1:
                    continue

                @pl.when(ok)
                def _(there=there):
                    b = there * 2 + 1 - self.lo
                    self.copy(b, 2, p).wait_recv()
                    if use is not None:
                        use(b, p)

    def drain(self):
        self.first(lambda c: c.wait_send())
        for d in range(1, self.nh):
            for p in range(self.parts):
                for route, there, ok in self.sides(d):

                    @pl.when(ok)
                    def _(route=route, there=there):
                        b = there * 2 + self.lo
                        pl.when(self.can(route))(lambda: self.copy(b, route, p).wait_send())
                        self.copy(b, 2, p).wait_send()


def layer_kernel(
    n, nt, heads, kvs, dheads,
    tok, gain_in, aq, ak, av, dq, dk, dv, dz, ao, do, ab, par, og_in, out,
    gain, og, kvw, in_sem, tokbuf, normed, wbuf, obuf, abbuf, acc, kvbuf, st, stbuf, o_loc, r_mat, joined, part, rsbuf,
    tok_s, tok_r, w_s, w_r, o_s, o_r, ab_s, ab_r, kv_s, kv_r, st_s, st_r, rs_s, rs_r,
):
    me, t = lax.axis_index("sp"), lax.axis_index("tp")
    rows, width = tok.shape
    kb = aq.shape[0]
    hd = HEAD_DIM
    aw, kw, dw = heads * hd, kvs * hd, dheads * hd
    mine = [(tok, tokbuf.at[t])]
    at = 0
    for w in (aq, dq, dk, dv, dz):
        mine.append((w, wbuf.at[me, :, pl.ds(at, w.shape[1])]))
        at += w.shape[1]
    mine += [(ak, kvw.at[pl.ds(0, kw)]), (av, kvw.at[pl.ds(kw, kw)]), (gain_in, gain), (og_in, og)]
    mine += [(ao, obuf.at[me, pl.ds(0, aw)]), (do, obuf.at[me, pl.ds(aw, dw)])]
    mine = [pltpu.make_async_copy(a, b, in_sem.at[i]) for i, (a, b) in enumerate(mine)]
    for c in mine:
        c.start()
    bar = pltpu.get_barrier_semaphore()
    for d in range(1, n):
        pl.semaphore_signal(bar, inc=1, device_id=(lax.rem(me + d, n), t), device_id_type=MESH)
    for d in range(1, nt):
        pl.semaphore_signal(bar, inc=1, device_id=(me, lax.rem(t + d, nt)), device_id_type=MESH)
    pl.semaphore_wait(bar, n - 1 + nt - 1)

    for c in mine:
        c.wait()
    wbuf[me, :, at:] = kvw[...].T
    tok_copies = [
        copy_to(tokbuf.at[t], tokbuf.at[t], tok_s.at[d - 1], tok_r.at[t], (me, lax.rem(t + d, nt)))
        for d in range(1, nt)
    ]
    for c in tok_copies:
        c.start()
    wg = Gather(n, me, t, wbuf, w_s, w_r, PARTS)
    ogather = Gather(n, me, t, obuf, o_s, o_r, 1)
    wg.begin()

    def ab_copy(d):
        p = lax.rem(me + d, n)
        return copy_to(ab, abbuf.at[me], ab_s.at[d], ab_r.at[me], (p, t))

    for d in range(1, n):
        ab_copy(d).start()
    abbuf[me] = ab[...]
    for d in range(1, nt):
        j = lax.rem(t + d, nt)
        copy_to(tokbuf.at[t], tokbuf.at[j], tok_s.at[d - 1], tok_r.at[j], (me, j)).wait_recv()
    total = jnp.zeros((rows, 1), F32)
    for j in range(nt):
        x = tokbuf[j].astype(F32)
        total += jnp.sum(x * x, axis=-1, keepdims=True)
    inverse = lax.rsqrt(total / (nt * width) + norm_eps)
    per = width // kb
    for j in range(nt):
        x = (tokbuf[j].astype(F32) * inverse * gain[:, j * width : (j + 1) * width]).astype(BF16)
        for i in range(per):
            normed[j * per + i] = x[:, i * kb : (i + 1) * kb]
    acc[...] = plain(normed[me], wbuf[me])

    half = wbuf.shape[2] // PARTS

    def use(b, p):
        cols = slice(p * half, (p + 1) * half)
        acc[:, cols] += plain(normed[b], wbuf[b, :, cols])

    for d in range(1, n // 2 + 1):
        wg.step(d, use)
    ogather.begin()

    kvbuf[WINDOW : WINDOW + rows] = acc[:, aw + 4 * dw :].astype(BF16)

    @pl.when(me == 0)
    def _():
        kvbuf[:WINDOW] = jnp.zeros((WINDOW, 2 * kw), BF16)

    @pl.when(me == n - 1)
    def _():
        kvbuf[WINDOW + rows :] = jnp.zeros((WINDOW, 2 * kw), BF16)

    base = aw
    for d in range(1, n):
        p = lax.rem(me + d, n)
        copy_to(ab, abbuf.at[p], ab_s.at[d], ab_r.at[p], (p, t)).wait_recv()
    tail = plain(abbuf[0], normed[0], ((1,), (1,)))
    for b in range(1, n):
        tail += plain(abbuf[b], normed[b], ((1,), (1,)))
    beta_t = jax.nn.sigmoid(tail + par[:, 0:1])
    soft = jnp.maximum(tail, 0.0) + jnp.log1p(jnp.exp(-jnp.abs(tail)))
    g_t = par[:, 1:2] * soft
    ri = lax.broadcasted_iota(jnp.int32, (rows, rows), 0)
    ci = lax.broadcasted_iota(jnp.int32, (rows, rows), 1)
    incl = (ri >= ci, ri <= ci)
    strict = (ri > ci, ri < ci)
    na = ab.shape[0]
    cum_t = [exact(g_t, jnp.where(m, 1.0, 0.0).astype(F32)) for m in (incl[1], incl[0])]
    stack = [beta_t] + cum_t
    if 3 * na < 128:
        stack.append(jnp.zeros((128 - 3 * na, rows), F32))
    columns = jnp.concatenate(stack, axis=0).T

    def head_to(p):
        up = copy_to(
            kvbuf.at[pl.ds(rows, WINDOW)], kvbuf.at[pl.ds(0, WINDOW)],
            kv_s.at[0], kv_r.at[0], (me + 1, t),
        )
        down = copy_to(
            kvbuf.at[pl.ds(WINDOW, WINDOW)], kvbuf.at[pl.ds(WINDOW + rows, WINDOW)],
            kv_s.at[1], kv_r.at[1], (me - 1, t),
        )
        return (up, down)[p]

    pl.when(me < n - 1)(lambda: head_to(0).start())
    pl.when(me > 0)(lambda: head_to(1).start())

    chains = []
    qs = []
    for h in range(dheads):
        def cols(i):
            lo_c = base + i * dw + h * hd
            return acc[:, lo_c : lo_c + hd].astype(BF16).astype(F32)

        q = unit_rows(silu(cols(0))) * hd ** (-0.5)
        k = unit_rows(silu(cols(1)))
        v = silu(cols(2))
        kk = near(k, k, ((1,), (1,)))
        qk = near(q, k, ((1,), (1,)))
        for r in range(2):
            c = h * 2 + r
            lane = 2 * dheads + c
            at = (1 + r) * na + lane
            gcol = columns[:, at : at + 1]
            grow = cum_t[r][lane : lane + 1, :]
            beta = columns[:, c : c + 1]
            decay = jnp.where(incl[r], jnp.exp(jnp.minimum(gcol - grow, 0.0)), 0.0)
            a = jnp.where(strict[r], beta * kk * decay, 0.0)
            eg = jnp.exp(gcol)
            last = gcol[rows - 1 : rows, :] if r == 0 else gcol[0:1, :]
            chains.append(
                dict(
                    r=r, h=h, a=a, rhs=jnp.concatenate([beta * v, beta * k * eg], axis=1),
                    pm=qk * decay, qe=q * eg, kd=(k * jnp.exp(last - gcol)).T, last=last,
                )
            )
    size = 1
    while (1 << size) <= rows:
        size += 1
    levels = size - 1
    eye = jnp.where(ri == ci, 1.0, 0.0).astype(F32)
    xor = ri ^ ci
    inv = [eye - jnp.where(xor == 1, ch["a"], 0.0) for ch in chains]
    pairs = [split(ch["a"]) for ch in chains]
    ogather.step(1)
    for lv in range(1, levels):
        m = jnp.where((xor >> lv) == 1, 1.0, 0.0).astype(BF16)
        xs = [split(x) for x in inv]
        left = [close(x, (m * a[0], m * a[1])) for x, a in zip(xs, pairs)]
        inv = [x - close(split(y), z) for x, y, z in zip(inv, left, xs)]
    sols = [split(close(split(x), split(ch["rhs"]))) for x, ch in zip(inv, chains)]
    outs = [close(split(ch["kd"]), s) for ch, s in zip(chains, sols)]
    e64 = jnp.where(
        lax.broadcasted_iota(jnp.int32, (hd, hd), 0)
        == lax.broadcasted_iota(jnp.int32, (hd, hd), 1), 1.0, 0.0,
    ).astype(F32)
    for ch, s in zip(chains, outs):
        full = jnp.concatenate([s[:, :hd], jnp.exp(ch["last"]) * e64 - s[:, hd:]], axis=1)
        st[ch["r"], ch["h"]] = full.astype(BF16)
    def state_copy(r, p):
        return copy_to(st.at[r], stbuf.at[me], st_s.at[p], st_r.at[me], (p, t))

    def state_all(act):
        for d in range(n - 1, 0, -1):
            pl.when(me + d < n)(lambda d=d: act(state_copy(0, me + d)))
            pl.when(me - d >= 0)(lambda d=d: act(state_copy(1, me - d)))

    state_all(lambda c: c.start())
    inner = [close(split(ch["pm"]), s) for ch, s in zip(chains, sols)]
    for ch, s in zip(chains, inner):
        o_loc[ch["r"], ch["h"]] = s[:, :hd]
        r_mat[ch["r"], ch["h"]] = ch["qe"] - s[:, hd:]


    ogather.step(2)

    pl.when(me > 0)(lambda: head_to(0).wait_recv())
    pl.when(me < n - 1)(lambda: head_to(1).wait_recv())
    span = rows + 2 * WINDOW
    qi = lax.broadcasted_iota(jnp.int32, (rows, span), 0)
    kj = lax.broadcasted_iota(jnp.int32, (rows, span), 1) - WINDOW
    pos = kj + me * rows
    allowed = (jnp.abs(qi - kj) <= WINDOW) & (pos >= 0) & (pos < n * rows)
    for h in range(heads):
        g = h // (heads // kvs)
        q = acc[:, h * hd : (h + 1) * hd].astype(BF16)
        s = plain(q, kvbuf[:, g * hd : (g + 1) * hd], ((1,), (1,))) * hd ** (-0.5)
        s = jnp.where(allowed, s, -jnp.inf)
        sink = par[h : h + 1, 2:3]
        m = jnp.maximum(jnp.max(s, axis=-1, keepdims=True), sink)
        e = jnp.exp(s - m)
        p = e / (jnp.sum(e, axis=-1, keepdims=True) + jnp.exp(sink - m))
        o = plain(p.astype(BF16), kvbuf[:, kw + g * hd : kw + (g + 1) * hd])
        joined[:, h * hd : (h + 1) * hd] = o.astype(BF16)
    for d in range(3, n // 2):
        ogather.step(d)

    for i in range(n):

        @pl.when(me != i)
        def _(i=i):
            copy_to(st.at[0], stbuf.at[i], st_s.at[i], st_r.at[i], (me, t)).wait_recv()

    fore = [jnp.zeros((hd, hd), F32)] * dheads
    back = [jnp.zeros((hd, hd), F32)] * dheads

    def enter(i, state, h, ok):
        both = jnp.where(ok, stbuf[i, h].astype(F32), ident)
        move, (high, low) = both[:, hd:].astype(BF16), split(state)
        return plain(move, high) + plain(move, low) + both[:, :hd]

    ident = jnp.concatenate([jnp.zeros((hd, hd), F32), e64], axis=1)
    for i in range(n - 1):
        fore = [enter(i, x, h, i < me) for h, x in enumerate(fore)]
        back = [enter(n - 1 - i, x, h, n - 1 - i > me) for h, x in enumerate(back)]
    if n // 2 > 2:
        ogather.step(n // 2)
    for h in range(dheads):
        o = o_loc[0, h] + o_loc[1, h] + near(r_mat[0, h], fore[h]) + near(r_mat[1, h], back[h])
        o = o * lax.rsqrt(jnp.mean(o * o, axis=-1, keepdims=True) + norm_eps) * og[...]
        lo_c = base + 3 * dw + h * hd
        gate = acc[:, lo_c : lo_c + hd].astype(BF16).astype(F32)
        joined[:, aw + h * hd : aw + (h + 1) * hd] = (o * silu(gate)).astype(BF16)

    cw = ao.shape[1]
    tr = rows // nt
    lhs = joined[...]
    for b in range(n):
        y = plain(lhs, obuf[b])
        for j in range(nt):
            part[j, :, b * cw : (b + 1) * cw] = y[j * tr : (j + 1) * tr].astype(SUM_DTYPE)
    rs_copies = [
        copy_to(
            part.at[lax.rem(t + d, nt)], rsbuf.at[d - 1], rs_s.at[d - 1], rs_r.at[d - 1],
            (me, lax.rem(t + d, nt)),
        )
        for d in range(1, nt)
    ]
    for c in rs_copies:
        c.start()
    own = joined[pl.ds(pl.multiple_of(t * tr, tr), tr)]
    for c in tok_copies:
        c.wait_send()
    for d in range(1, n):
        ab_copy(d).wait_send()
    wg.drain()
    ogather.drain()
    pl.when(me < n - 1)(lambda: head_to(0).wait_send())
    pl.when(me > 0)(lambda: head_to(1).wait_send())
    state_all(lambda c: c.wait_send())
    total = jnp.concatenate([plain(own, obuf[b]) for b in range(n)], axis=1)
    for d in range(1, nt):
        rs_copies[d - 1].wait_recv()
        total += rsbuf[d - 1].astype(F32)
    out[...] = total.astype(BF16)
    for c in rs_copies:
        c.wait_send()


def per_device(
    tokens, norm_gain, attn_query, attn_key, attn_value, sink_logit, delta_query, delta_key,
    delta_value, delta_gate, beta_weight, decay_weight, beta_shift, decay_log, out_gain,
    attn_out, delta_out,
):
    n, nt = lax.axis_size("sp"), lax.axis_size("tp")
    rows, width = tokens.shape
    kb = attn_query.shape[0]
    heads, kvs = attn_query.shape[1] // HEAD_DIM, attn_key.shape[1] // HEAD_DIM
    dheads = delta_query.shape[1] // HEAD_DIM
    ab = 2 * dheads
    wide = (2 * kvs + heads + 4 * dheads) * HEAD_DIM
    na = -(-2 * ab // 16) * 16
    gates = jnp.concatenate(
        [
            beta_weight.reshape(kb, ab).T, decay_weight.reshape(kb, ab).T,
            jnp.zeros((na - 2 * ab, kb), BF16),
        ],
        axis=0,
    )
    flat = lambda a, before: jnp.pad(a, (before, na - before - a.shape[0]))
    par = jnp.stack(
        [
            flat(beta_shift.T.reshape(ab), 0),
            flat(-jnp.exp(decay_log.T.reshape(ab)) / (rows * n), ab),
            flat(sink_logit, 0),
        ],
        axis=1,
    )
    cw = attn_out.shape[1]
    tr = rows // nt
    hd = HEAD_DIM
    kw = kvs * hd
    dma = pltpu.SemaphoreType.DMA
    vm = pl.BlockSpec(memory_space=pltpu.VMEM)
    hbm = pl.BlockSpec(memory_space=pltpu.HBM)
    return pl.pallas_call(
        functools.partial(layer_kernel, n, nt, heads, kvs, dheads),
        out_shape=jax.ShapeDtypeStruct((tr, n * cw), BF16),
        in_specs=[hbm] * 11 + [vm] * 2 + [hbm],
        out_specs=vm,
        scratch_shapes=[
            pltpu.VMEM((1, nt * width), F32),
            pltpu.VMEM((1, hd), F32),
            pltpu.VMEM((2 * kw, kb), BF16),
            dma((12,)),
            pltpu.VMEM((nt, rows, width), BF16),
            pltpu.VMEM((n, rows, kb), BF16),
            pltpu.VMEM((n, kb, wide), BF16),
            pltpu.VMEM((n, (heads + dheads) * hd, cw), BF16),
            pltpu.VMEM((n, na, kb), BF16),
            pltpu.VMEM((rows, wide), F32),
            pltpu.VMEM((rows + 2 * WINDOW, 2 * kw), BF16),
            pltpu.VMEM((2, dheads, hd, 2 * hd), BF16),
            pltpu.VMEM((n, dheads, hd, 2 * hd), BF16),
            pltpu.VMEM((2, dheads, rows, hd), F32),
            pltpu.VMEM((2, dheads, rows, hd), F32),
            pltpu.VMEM((rows, (heads + dheads) * hd), BF16),
            pltpu.VMEM((nt, tr, n * cw), SUM_DTYPE),
            pltpu.VMEM((nt - 1, tr, n * cw), SUM_DTYPE),
            dma((nt - 1,)), dma((nt,)),
            dma((3, n, PARTS)), dma((n, PARTS)),
            dma((3, n, 1)), dma((n, 1)),
            dma((n,)), dma((n,)),
            dma((2,)), dma((2,)),
            dma((n,)), dma((n,)),
            dma((nt - 1,)), dma((nt - 1,)),
        ],
        compiler_params=pltpu.CompilerParams(
            collective_id=0, has_side_effects=True, vmem_limit_bytes=60 * 1024 * 1024
        ),
    )(
        tokens, norm_gain.reshape(1, nt * width), attn_query, attn_key.T, attn_value.T, delta_query,
        delta_key, delta_value, delta_gate, attn_out, delta_out, gates, par,
        out_gain.reshape(1, hd),
    )


def solution(mesh):
    return jax.shard_map(
        per_device,
        mesh=mesh,
        in_specs=(
            P("sp", "tp"), P(), P("sp", "tp"), P("sp", "tp"), P("sp", "tp"), P("tp"),
            P("sp", "tp"), P("sp", "tp"), P("sp", "tp"), P("sp", "tp"),
            P("sp", "tp", None), P("sp", "tp", None), P(None, "tp"), P(None, "tp"), P(),
            P("tp", "sp"), P("tp", "sp"),
        ),
        out_specs=P(("sp", "tp"), None),
        check_vma=False,
    )
```

```python
import functools

import jax
import jax.numpy as jnp
from jax import lax
from jax.experimental import pallas as pl
from jax.experimental.pallas import tpu as pltpu
from jax.sharding import PartitionSpec as P

HEAD_DIM = 64
WINDOW = 64
norm_eps = 1e-06
MESH = pl.DeviceIdType.MESH
F32 = jnp.float32
BF16 = jnp.bfloat16
SUM_DTYPE = jnp.bfloat16
PARTS = 3


def exact(a, b, dims=((1,), (0,))):
    return lax.dot_general(
        a, b, (dims, ((), ())), precision=lax.Precision.HIGHEST, preferred_element_type=F32
    )


def plain(a, b, dims=((1,), (0,))):
    return lax.dot_general(a, b, (dims, ((), ())), preferred_element_type=F32)


def split(x):
    high = x.astype(BF16)
    return high, (x - high.astype(F32)).astype(BF16)


def close(a, b, dims=((1,), (0,))):
    (ca,), (cb,) = dims
    left = jnp.concatenate([a[0], a[1], a[0]], axis=ca)
    right = jnp.concatenate([b[0], b[0], b[1]], axis=cb)
    return plain(left, right, dims)


def near(a, b, dims=((1,), (0,))):
    a, b = split(a), split(b)
    return plain(a[0], b[0], dims) + (plain(a[1], b[0], dims) + plain(a[0], b[1], dims))


def silu(x):
    return x * jax.nn.sigmoid(x)


def unit_rows(x):
    return x * lax.rsqrt(jnp.sum(x * x, axis=-1, keepdims=True) + norm_eps)


def copy_to(src, dst, send, recv, device):
    return pltpu.make_async_remote_copy(
        src_ref=src,
        dst_ref=dst,
        send_sem=send,
        recv_sem=recv,
        device_id=device,
        device_id_type=MESH,
    )


class Gather:
    def __init__(self, n, me, tp, buf, send, recv, parts):
        self.nh = n // 2
        self.me, self.tp = me, tp
        self.lo, self.hi = lax.rem(me, 2), lax.div(me, 2)
        self.buf, self.send, self.recv = buf, send, recv
        self.parts = parts
        self.size = buf.shape[2] // parts

    def copy(self, b, route, p):
        target = (self.me + 2, self.me - 2, self.hi * 2 + 1 - self.lo)[route]
        cols = pl.ds(p * self.size, self.size)
        return copy_to(
            self.buf.at[b, :, cols],
            self.buf.at[b, :, cols],
            self.send.at[route, b, p],
            self.recv.at[b, p],
            (target, self.tp),
        )

    def can(self, route):
        return self.hi < self.nh - 1 if route == 0 else self.hi > 0

    def first(self, act):
        for p in range(self.parts):
            for route in (0, 1):
                pl.when(self.can(route))(lambda p=p, route=route: act(self.copy(self.me, route, p)))
            act(self.copy(self.me, 2, p))

    def begin(self):
        self.first(lambda c: c.start())

    def sides(self, d):
        return ((0, self.hi - d, self.hi - d >= 0), (1, self.hi + d, self.hi + d < self.nh))

    def step(self, d, use=None):
        for p in range(self.parts):
            if d < self.nh:
                for route, there, ok in self.sides(d):

                    @pl.when(ok)
                    def _(route=route, there=there):
                        b = there * 2 + self.lo
                        self.copy(b, 2, p).wait_recv()
                        pl.when(self.can(route))(lambda: self.copy(b, route, p).start())
                        self.copy(b, 2, p).start()
                        if use is not None:
                            use(b, p)

            for i, (_, there, ok) in enumerate(self.sides(d - 1)):
                if d == 1 and i == 1:
                    continue

                @pl.when(ok)
                def _(there=there):
                    b = there * 2 + 1 - self.lo
                    self.copy(b, 2, p).wait_recv()
                    if use is not None:
                        use(b, p)

    def drain(self):
        self.first(lambda c: c.wait_send())
        for d in range(1, self.nh):
            for p in range(self.parts):
                for route, there, ok in self.sides(d):

                    @pl.when(ok)
                    def _(route=route, there=there):
                        b = there * 2 + self.lo
                        pl.when(self.can(route))(lambda: self.copy(b, route, p).wait_send())
                        self.copy(b, 2, p).wait_send()


def layer_kernel(
    n, nt, heads, kvs, dheads,
    tok, gain_in, aq, ak, av, dq, dk, dv, dz, ao, do, ab, par, og_in, out,
    gain, og, kvw, in_sem, tokbuf, normed, wbuf, obuf, abbuf, acc, kvbuf, st, stbuf, o_loc, r_mat, joined, part, rsbuf,
    tok_s, tok_r, w_s, w_r, o_s, o_r, ab_s, ab_r, kv_s, kv_r, st_s, st_r, rs_s, rs_r,
):
    me, t = lax.axis_index("sp"), lax.axis_index("tp")
    rows, width = tok.shape
    kb = aq.shape[0]
    hd = HEAD_DIM
    aw, kw, dw = heads * hd, kvs * hd, dheads * hd
    mine = [(tok, tokbuf.at[t])]
    at = 0
    for w in (aq, dq, dk, dv, dz):
        mine.append((w, wbuf.at[me, :, pl.ds(at, w.shape[1])]))
        at += w.shape[1]
    mine += [(ak, kvw.at[pl.ds(0, kw)]), (av, kvw.at[pl.ds(kw, kw)]), (gain_in, gain), (og_in, og)]
    mine += [(ao, obuf.at[me, pl.ds(0, aw)]), (do, obuf.at[me, pl.ds(aw, dw)])]
    mine = [pltpu.make_async_copy(a, b, in_sem.at[i]) for i, (a, b) in enumerate(mine)]
    for c in mine:
        c.start()
    bar = pltpu.get_barrier_semaphore()
    for d in range(1, n):
        pl.semaphore_signal(bar, inc=1, device_id=(lax.rem(me + d, n), t), device_id_type=MESH)
    for d in range(1, nt):
        pl.semaphore_signal(bar, inc=1, device_id=(me, lax.rem(t + d, nt)), device_id_type=MESH)
    pl.semaphore_wait(bar, n - 1 + nt - 1)

    for c in mine:
        c.wait()
    wbuf[me, :, at:] = kvw[...].T
    tok_copies = [
        copy_to(tokbuf.at[t], tokbuf.at[t], tok_s.at[d - 1], tok_r.at[t], (me, lax.rem(t + d, nt)))
        for d in range(1, nt)
    ]
    for c in tok_copies:
        c.start()
    wg = Gather(n, me, t, wbuf, w_s, w_r, PARTS)
    ogather = Gather(n, me, t, obuf, o_s, o_r, 1)
    wg.begin()

    def ab_copy(d):
        p = lax.rem(me + d, n)
        return copy_to(ab, abbuf.at[me], ab_s.at[d], ab_r.at[me], (p, t))

    for d in range(1, n):
        ab_copy(d).start()
    abbuf[me] = ab[...]
    for d in range(1, nt):
        j = lax.rem(t + d, nt)
        copy_to(tokbuf.at[t], tokbuf.at[j], tok_s.at[d - 1], tok_r.at[j], (me, j)).wait_recv()
    total = jnp.zeros((rows, 1), F32)
    for j in range(nt):
        x = tokbuf[j].astype(F32)
        total += jnp.sum(x * x, axis=-1, keepdims=True)
    inverse = lax.rsqrt(total / (nt * width) + norm_eps)
    per = width // kb
    for j in range(nt):
        x = (tokbuf[j].astype(F32) * inverse * gain[:, j * width : (j + 1) * width]).astype(BF16)
        for i in range(per):
            normed[j * per + i] = x[:, i * kb : (i + 1) * kb]
    acc[...] = plain(normed[me], wbuf[me])

    half = wbuf.shape[2] // PARTS

    def use(b, p):
        cols = slice(p * half, (p + 1) * half)
        acc[:, cols] += plain(normed[b], wbuf[b, :, cols])

    for d in range(1, n // 2 + 1):
        wg.step(d, use)
    ogather.begin()

    kvbuf[WINDOW : WINDOW + rows] = acc[:, aw + 4 * dw :].astype(BF16)

    @pl.when(me == 0)
    def _():
        kvbuf[:WINDOW] = jnp.zeros((WINDOW, 2 * kw), BF16)

    @pl.when(me == n - 1)
    def _():
        kvbuf[WINDOW + rows :] = jnp.zeros((WINDOW, 2 * kw), BF16)

    base = aw
    for d in range(1, n):
        p = lax.rem(me + d, n)
        copy_to(ab, abbuf.at[p], ab_s.at[d], ab_r.at[p], (p, t)).wait_recv()
    tail = plain(abbuf[0], normed[0], ((1,), (1,)))
    for b in range(1, n):
        tail += plain(abbuf[b], normed[b], ((1,), (1,)))
    beta_t = jax.nn.sigmoid(tail + par[:, 0:1])
    soft = jnp.maximum(tail, 0.0) + jnp.log1p(jnp.exp(-jnp.abs(tail)))
    g_t = par[:, 1:2] * soft
    ri = lax.broadcasted_iota(jnp.int32, (rows, rows), 0)
    ci = lax.broadcasted_iota(jnp.int32, (rows, rows), 1)
    incl = (ri >= ci, ri <= ci)
    strict = (ri > ci, ri < ci)
    na = ab.shape[0]
    cum_t = [exact(g_t, jnp.where(m, 1.0, 0.0).astype(F32)) for m in (incl[1], incl[0])]
    stack = [beta_t] + cum_t
    if 3 * na < 128:
        stack.append(jnp.zeros((128 - 3 * na, rows), F32))
    columns = jnp.concatenate(stack, axis=0).T

    def head_to(p):
        up = copy_to(
            kvbuf.at[pl.ds(rows, WINDOW)], kvbuf.at[pl.ds(0, WINDOW)],
            kv_s.at[0], kv_r.at[0], (me + 1, t),
        )
        down = copy_to(
            kvbuf.at[pl.ds(WINDOW, WINDOW)], kvbuf.at[pl.ds(WINDOW + rows, WINDOW)],
            kv_s.at[1], kv_r.at[1], (me - 1, t),
        )
        return (up, down)[p]

    pl.when(me < n - 1)(lambda: head_to(0).start())
    pl.when(me > 0)(lambda: head_to(1).start())

    chains = []
    qs = []
    for h in range(dheads):
        def cols(i):
            lo_c = base + i * dw + h * hd
            return acc[:, lo_c : lo_c + hd].astype(BF16).astype(F32)

        q = unit_rows(silu(cols(0))) * hd ** (-0.5)
        k = unit_rows(silu(cols(1)))
        v = silu(cols(2))
        kk = near(k, k, ((1,), (1,)))
        qk = near(q, k, ((1,), (1,)))
        for r in range(2):
            c = h * 2 + r
            lane = 2 * dheads + c
            at = (1 + r) * na + lane
            gcol = columns[:, at : at + 1]
            grow = cum_t[r][lane : lane + 1, :]
            beta = columns[:, c : c + 1]
            decay = jnp.where(incl[r], jnp.exp(jnp.minimum(gcol - grow, 0.0)), 0.0)
            a = jnp.where(strict[r], beta * kk * decay, 0.0)
            eg = jnp.exp(gcol)
            last = gcol[rows - 1 : rows, :] if r == 0 else gcol[0:1, :]
            chains.append(
                dict(
                    r=r, h=h, a=a, rhs=jnp.concatenate([beta * v, beta * k * eg], axis=1),
                    pm=qk * decay, qe=q * eg, kd=(k * jnp.exp(last - gcol)).T, last=last,
                )
            )
    size = 1
    while (1 << size) <= rows:
        size += 1
    levels = size - 1
    eye = jnp.where(ri == ci, 1.0, 0.0).astype(F32)
    xor = ri ^ ci
    inv = [eye - jnp.where(xor == 1, ch["a"], 0.0) for ch in chains]
    pairs = [split(ch["a"]) for ch in chains]
    ogather.step(1)
    for lv in range(1, levels):
        m = jnp.where((xor >> lv) == 1, 1.0, 0.0).astype(BF16)
        xs = [split(x) for x in inv]
        left = [close(x, (m * a[0], m * a[1])) for x, a in zip(xs, pairs)]
        inv = [x - close(split(y), z) for x, y, z in zip(inv, left, xs)]
    sols = [split(close(split(x), split(ch["rhs"]))) for x, ch in zip(inv, chains)]
    outs = [close(split(ch["kd"]), s) for ch, s in zip(chains, sols)]
    e64 = jnp.where(
        lax.broadcasted_iota(jnp.int32, (hd, hd), 0)
        == lax.broadcasted_iota(jnp.int32, (hd, hd), 1), 1.0, 0.0,
    ).astype(F32)
    for ch, s in zip(chains, outs):
        full = jnp.concatenate([s[:, :hd], jnp.exp(ch["last"]) * e64 - s[:, hd:]], axis=1)
        st[ch["r"], ch["h"]] = full.astype(BF16)
    def state_copy(r, p):
        return copy_to(st.at[r], stbuf.at[me], st_s.at[p], st_r.at[me], (p, t))

    def state_all(act):
        for d in range(n - 1, 0, -1):
            pl.when(me + d < n)(lambda d=d: act(state_copy(0, me + d)))
            pl.when(me - d >= 0)(lambda d=d: act(state_copy(1, me - d)))

    state_all(lambda c: c.start())
    inner = [close(split(ch["pm"]), s) for ch, s in zip(chains, sols)]
    for ch, s in zip(chains, inner):
        o_loc[ch["r"], ch["h"]] = s[:, :hd]
        r_mat[ch["r"], ch["h"]] = ch["qe"] - s[:, hd:]


    ogather.step(2)

    pl.when(me > 0)(lambda: head_to(0).wait_recv())
    pl.when(me < n - 1)(lambda: head_to(1).wait_recv())
    span = rows + 2 * WINDOW
    qi = lax.broadcasted_iota(jnp.int32, (rows, span), 0)
    kj = lax.broadcasted_iota(jnp.int32, (rows, span), 1) - WINDOW
    pos = kj + me * rows
    allowed = (jnp.abs(qi - kj) <= WINDOW) & (pos >= 0) & (pos < n * rows)
    for h in range(heads):
        g = h // (heads // kvs)
        q = acc[:, h * hd : (h + 1) * hd].astype(BF16)
        s = plain(q, kvbuf[:, g * hd : (g + 1) * hd], ((1,), (1,))) * hd ** (-0.5)
        s = jnp.where(allowed, s, -jnp.inf)
        sink = par[h : h + 1, 2:3]
        m = jnp.maximum(jnp.max(s, axis=-1, keepdims=True), sink)
        e = jnp.exp(s - m)
        p = e / (jnp.sum(e, axis=-1, keepdims=True) + jnp.exp(sink - m))
        o = plain(p.astype(BF16), kvbuf[:, kw + g * hd : kw + (g + 1) * hd])
        joined[:, h * hd : (h + 1) * hd] = o.astype(BF16)
    for d in range(3, n // 2):
        ogather.step(d)

    for i in range(n):

        @pl.when(me != i)
        def _(i=i):
            copy_to(st.at[0], stbuf.at[i], st_s.at[i], st_r.at[i], (me, t)).wait_recv()

    fore = [jnp.zeros((hd, hd), F32)] * dheads
    back = [jnp.zeros((hd, hd), F32)] * dheads

    def enter(i, state, h, ok):
        both = jnp.where(ok, stbuf[i, h].astype(F32), ident)
        move, (high, low) = both[:, hd:].astype(BF16), split(state)
        return plain(move, high) + plain(move, low) + both[:, :hd]

    ident = jnp.concatenate([jnp.zeros((hd, hd), F32), e64], axis=1)
    for i in range(n - 1):
        fore = [enter(i, x, h, i < me) for h, x in enumerate(fore)]
        back = [enter(n - 1 - i, x, h, n - 1 - i > me) for h, x in enumerate(back)]
    if n // 2 > 2:
        ogather.step(n // 2)
    for h in range(dheads):
        o = o_loc[0, h] + o_loc[1, h] + near(r_mat[0, h], fore[h]) + near(r_mat[1, h], back[h])
        o = o * lax.rsqrt(jnp.mean(o * o, axis=-1, keepdims=True) + norm_eps) * og[...]
        lo_c = base + 3 * dw + h * hd
        gate = acc[:, lo_c : lo_c + hd].astype(BF16).astype(F32)
        joined[:, aw + h * hd : aw + (h + 1) * hd] = (o * silu(gate)).astype(BF16)

    cw = ao.shape[1]
    tr = rows // nt
    lhs = joined[...]
    for b in range(n):
        y = plain(lhs, obuf[b])
        for j in range(nt):
            part[j, :, b * cw : (b + 1) * cw] = y[j * tr : (j + 1) * tr].astype(SUM_DTYPE)
    rs_copies = [
        copy_to(
            part.at[lax.rem(t + d, nt)], rsbuf.at[d - 1], rs_s.at[d - 1], rs_r.at[d - 1],
            (me, lax.rem(t + d, nt)),
        )
        for d in range(1, nt)
    ]
    for c in rs_copies:
        c.start()
    for c in tok_copies:
        c.wait_send()
    for d in range(1, n):
        ab_copy(d).wait_send()
    wg.drain()
    ogather.drain()
    pl.when(me < n - 1)(lambda: head_to(0).wait_send())
    pl.when(me > 0)(lambda: head_to(1).wait_send())
    state_all(lambda c: c.wait_send())
    total = part[t].astype(F32)
    for d in range(1, nt):
        rs_copies[d - 1].wait_recv()
        total += rsbuf[d - 1].astype(F32)
    out[...] = total.astype(BF16)
    for c in rs_copies:
        c.wait_send()


def per_device(
    tokens, norm_gain, attn_query, attn_key, attn_value, sink_logit, delta_query, delta_key,
    delta_value, delta_gate, beta_weight, decay_weight, beta_shift, decay_log, out_gain,
    attn_out, delta_out,
):
    n, nt = lax.axis_size("sp"), lax.axis_size("tp")
    rows, width = tokens.shape
    kb = attn_query.shape[0]
    heads, kvs = attn_query.shape[1] // HEAD_DIM, attn_key.shape[1] // HEAD_DIM
    dheads = delta_query.shape[1] // HEAD_DIM
    ab = 2 * dheads
    wide = (2 * kvs + heads + 4 * dheads) * HEAD_DIM
    na = -(-2 * ab // 16) * 16
    gates = jnp.concatenate(
        [
            beta_weight.reshape(kb, ab).T, decay_weight.reshape(kb, ab).T,
            jnp.zeros((na - 2 * ab, kb), BF16),
        ],
        axis=0,
    )
    flat = lambda a, before: jnp.pad(a, (before, na - before - a.shape[0]))
    par = jnp.stack(
        [
            flat(beta_shift.T.reshape(ab), 0),
            flat(-jnp.exp(decay_log.T.reshape(ab)) / (rows * n), ab),
            flat(sink_logit, 0),
        ],
        axis=1,
    )
    cw = attn_out.shape[1]
    tr = rows // nt
    hd = HEAD_DIM
    kw = kvs * hd
    dma = pltpu.SemaphoreType.DMA
    vm = pl.BlockSpec(memory_space=pltpu.VMEM)
    hbm = pl.BlockSpec(memory_space=pltpu.HBM)
    return pl.pallas_call(
        functools.partial(layer_kernel, n, nt, heads, kvs, dheads),
        out_shape=jax.ShapeDtypeStruct((tr, n * cw), BF16),
        in_specs=[hbm] * 11 + [vm] * 2 + [hbm],
        out_specs=vm,
        scratch_shapes=[
            pltpu.VMEM((1, nt * width), F32),
            pltpu.VMEM((1, hd), F32),
            pltpu.VMEM((2 * kw, kb), BF16),
            dma((12,)),
            pltpu.VMEM((nt, rows, width), BF16),
            pltpu.VMEM((n, rows, kb), BF16),
            pltpu.VMEM((n, kb, wide), BF16),
            pltpu.VMEM((n, (heads + dheads) * hd, cw), BF16),
            pltpu.VMEM((n, na, kb), BF16),
            pltpu.VMEM((rows, wide), F32),
            pltpu.VMEM((rows + 2 * WINDOW, 2 * kw), BF16),
            pltpu.VMEM((2, dheads, hd, 2 * hd), BF16),
            pltpu.VMEM((n, dheads, hd, 2 * hd), BF16),
            pltpu.VMEM((2, dheads, rows, hd), F32),
            pltpu.VMEM((2, dheads, rows, hd), F32),
            pltpu.VMEM((rows, (heads + dheads) * hd), BF16),
            pltpu.VMEM((nt, tr, n * cw), SUM_DTYPE),
            pltpu.VMEM((nt - 1, tr, n * cw), SUM_DTYPE),
            dma((nt - 1,)), dma((nt,)),
            dma((3, n, PARTS)), dma((n, PARTS)),
            dma((3, n, 1)), dma((n, 1)),
            dma((n,)), dma((n,)),
            dma((2,)), dma((2,)),
            dma((n,)), dma((n,)),
            dma((nt - 1,)), dma((nt - 1,)),
        ],
        compiler_params=pltpu.CompilerParams(
            collective_id=0, has_side_effects=True, vmem_limit_bytes=60 * 1024 * 1024
        ),
    )(
        tokens, norm_gain.reshape(1, nt * width), attn_query, attn_key.T, attn_value.T, delta_query,
        delta_key, delta_value, delta_gate, attn_out, delta_out, gates, par,
        out_gain.reshape(1, hd),
    )


def solution(mesh):
    return jax.shard_map(
        per_device,
        mesh=mesh,
        in_specs=(
            P("sp", "tp"), P(), P("sp", "tp"), P("sp", "tp"), P("sp", "tp"), P("tp"),
            P("sp", "tp"), P("sp", "tp"), P("sp", "tp"), P("sp", "tp"),
            P("sp", "tp", None), P("sp", "tp", None), P(None, "tp"), P(None, "tp"), P(),
            P("tp", "sp"), P("tp", "sp"),
        ),
        out_specs=P(("sp", "tp"), None),
        check_vma=False,
    )
```
